256 devices in a mesh: sp: 32 (over z, x), tp: 8 (over y, core).
Axes of the slice: x: 4, y: 4, z: 8, core: 2. Of those that a mesh axis runs over, the one named last changes fastest.
Arguments:
- hidden_in: bfloat16 [12288, 2048], P('sp', 'tp'), may hold values from -6 to 6
- in_gain: float32 [2048], replicated, may hold values from 0.1 to 1.9
- receptance_weight: bfloat16 [2048, 1024], P(None, 'tp'), may hold values from -0.125 to 0.125
- key_weight: bfloat16 [2048, 1024], P(None, 'tp'), may hold values from -0.125 to 0.125
- value_weight: bfloat16 [2048, 1024], P(None, 'tp'), may hold values from -0.125 to 0.125
- decay_down: bfloat16 [2048, 128], replicated, may hold values from -0.125 to 0.125
- decay_up: bfloat16 [128, 1024], P(None, 'tp'), may hold values from -0.5 to 0.5
- decay_base: float32 [1024], P('tp'), may hold values from -14 to -2
- decay_shift: float32 [12288, 1024], P('sp', 'tp'), may hold values from -1 to 0
- learn_rate: float32 [1024], P('tp'), may hold values from 0 to 1
- query_pair: bfloat16 [2048, 8, 128], P(None, 'tp'), may hold values from -1 to 1
- key_pair: bfloat16 [2048, 8, 128], P(None, 'tp'), may hold values from -1 to 1
- value_pair: bfloat16 [2048, 8, 128], P(None, 'tp'), may hold values from -0.125 to 0.125
- mix_lambda: float32 [8], P('tp'), may hold values from 0.3 to 0.8
- out_recurrent: bfloat16 [1024, 2048], P('tp'), may hold values from -0.1875 to 0.1875
- out_attention: bfloat16 [1024, 2048], P('tp'), may hold values from -0.1875 to 0.1875
- out_gain: float32 [2048], replicated, may hold values from 0.1 to 1.9
Outputs:
- layer_out: bfloat16 [12288, 2048], P(('sp', 'tp'))
- log_sums: float32 [8, 2, 12288], P('tp', None, 'sp')
The draws below stay inside these ranges and needn't reach their ends.
All inputs are finite; a program needn't handle non-finite values.
Results may differ from the reference program's by a relative error of at most 0.018.
Values may be sent and summed in bfloat16 or wider, within the bound.
A program may use at most 128 MiB of HBM per device.

```python
import math
import jax
import jax.numpy as jnp
from jax import lax

D = 2048
RH = 16
DH = 8
HD = 64
LOW = 128
TOK_DEV = 384
TOKENS = 12288
RD = 1024
DW = 1024


def paired_maps(key):
    base = jax.random.fold_in(key, 101)
    leading = jax.random.normal(jax.random.fold_in(base, 1), (D, DH, 2 * HD), jnp.float32) * (3.0 / D) ** 0.5
    trailing = jax.random.normal(jax.random.fold_in(base, 2), (D, DH, 2 * HD), jnp.float32) * D ** (-0.5)
    return (jnp.clip(leading, -1.0, 1.0), jnp.clip(trailing, -1.0, 1.0))


def draw_query_pair(key, part):
    return paired_maps(key)[0].astype(jnp.bfloat16)


def draw_key_pair(key, part):
    return paired_maps(key)[1].astype(jnp.bfloat16)


def draw_hidden_in(key, part):
    rows = jax.random.normal(jax.random.fold_in(key, 7), (TOKENS, D), jnp.float32)
    return jnp.clip(rows, -6.0, 6.0).astype(jnp.bfloat16)


def draw_decay_base(key, part):
    base = jax.random.fold_in(key, 23)
    share = 0.5
    slow = jax.random.uniform(jax.random.fold_in(base, 1), (RH, 1), jnp.float32) < share
    slow_level = jnp.log(jax.random.uniform(jax.random.fold_in(base, 2), (RH, HD), jnp.float32, 0.05, 0.25) / TOKENS)
    fast_level = jax.random.uniform(jax.random.fold_in(base, 3), (RH, HD), jnp.float32, -3.5, -2.0)
    return jnp.where(slow, slow_level, fast_level).reshape(RH * HD)


def draw_decay_shift(key, part):
    base = jax.random.fold_in(key, 31)
    block_total = TOKENS // TOK_DEV
    rates = jnp.exp(jax.random.uniform(jax.random.fold_in(base, 1), (block_total, 1, 1), jnp.float32, math.log(0.1), math.log(0.4))) / TOKENS
    steady = jnp.broadcast_to(rates, (block_total, TOK_DEV, RH * HD)).reshape(TOKENS, RH * HD)
    places = jax.random.randint(jax.random.fold_in(base, 2), (3,), 0, TOKENS)
    sizes = jax.random.uniform(jax.random.fold_in(base, 3), (3, RH * HD), jnp.float32, 0.22, 0.3)
    hits = (jnp.arange(TOKENS)[:, None] == places[None, :]).astype(jnp.float32)
    return -(steady + jnp.dot(hits, sizes))


def draw_learn_rate(key, part):
    base = jax.random.fold_in(key, 41)
    weak_level = jax.random.uniform(jax.random.fold_in(base, 1), (RH * HD,), jnp.float32, math.log(4.0), math.log(40.0))
    weak = jnp.exp(weak_level) / TOKENS
    strong = jnp.exp(jax.random.uniform(jax.random.fold_in(base, 2), (RH * HD,), jnp.float32, math.log(0.05), math.log(0.8)))
    picked = jax.random.randint(jax.random.fold_in(base, 3), (RH * HD,), 0, 8) < 5
    return jnp.where(picked, strong, weak)


def block_levels(rng, dims, shards, smallest, top_value):
    def one(position, blocks):
        heights = jax.random.uniform(jax.random.fold_in(jax.random.fold_in(rng, 6), position), (blocks,), jnp.float32, smallest / len(shards), top_value / len(shards))
        return jnp.repeat(jnp.exp(heights), dims[position] // blocks).reshape((-1,) + (1,) * (len(dims) - position - 1))

    level = one(*shards[0])
    for cut in shards[1:]:
        level = level * one(*cut)
    return level


def bell_draw(key, dims, scale, reach, pieces=(), held_as=jnp.bfloat16):
    values = scale * jax.random.normal(key, dims, jnp.float32)
    if pieces:
        values = values * block_levels(key, dims, pieces, -0.22, 0.18)
    return jnp.clip(values, -reach, reach).astype(held_as)


def setup_inputs(seed: int = 0) -> dict:
    key_list = jax.random.split(jax.random.key(seed), 18)
    return {
        "hidden_in": draw_hidden_in(jax.random.fold_in(key_list[17], 71), 0),
        "in_gain": jnp.clip(1.0 + 0.18 * jax.random.normal(key_list[1], (D,), jnp.float32), 0.1, 1.9),
        "receptance_weight": bell_draw(key_list[2], (D, RD), D ** -0.5, 0.125, ((1, 8),)),
        "key_weight": bell_draw(key_list[3], (D, RD), D ** -0.5, 0.125, ((1, 8),)),
        "value_weight": bell_draw(key_list[4], (D, RD), D ** -0.5, 0.125, ((1, 8),)),
        "decay_down": bell_draw(key_list[5], (D, LOW), D ** -0.5, 0.125),
        "decay_up": bell_draw(key_list[6], (LOW, RD), LOW ** -0.5, 0.5, ((1, 8),)),
        "decay_base": draw_decay_base(jax.random.fold_in(key_list[17], 71), 0),
        "decay_shift": draw_decay_shift(jax.random.fold_in(key_list[17], 71), 0),
        "learn_rate": draw_learn_rate(jax.random.fold_in(key_list[17], 71), 0),
        "query_pair": draw_query_pair(jax.random.fold_in(key_list[17], 71), 0),
        "key_pair": draw_key_pair(jax.random.fold_in(key_list[17], 71), 0),
        "value_pair": bell_draw(key_list[12], (D, DH, 2 * HD), D ** -0.5, 0.125, ((1, 8),)),
        "mix_lambda": jnp.clip(0.3 + 0.5 * jax.random.uniform(key_list[13], (DH,), jnp.float32) ** block_levels(key_list[13], (DH,), ((0, 8),), -0.2, 0.2), 0.3, 0.8),
        "out_recurrent": bell_draw(key_list[14], (RD, D), RD ** -0.5, 0.1875, ((0, 8),)),
        "out_attention": bell_draw(key_list[15], (DW, D), DW ** -0.5, 0.1875, ((0, 8),)),
        "out_gain": jnp.clip(1.0 + 0.18 * jax.random.normal(key_list[16], (D,), jnp.float32), 0.1, 1.9),
    }


HIGHEST = lax.Precision.HIGHEST
DECAY_SCALE = math.exp(-0.5)
NORM_EPS = 1e-06
GROUP_EPS = 0.00064
HEAD_EPS = 1e-05
KEY_EPS = 1e-06

def rms_rows(values, gain):
    wide = values.astype(jnp.float32)
    return wide * lax.rsqrt(lax.optimization_barrier(jnp.mean(wide * wide, axis=-1, keepdims=True)) + NORM_EPS) * gain

def project(normed, weight):
    return jnp.dot(normed, weight.reshape(D, -1), preferred_element_type=jnp.float32).astype(jnp.bfloat16)

def recurrence(receptance, key_rows, value_rows, log_decay, learn_rate):
    shape = (TOKENS, RH, HD)
    receptance = receptance.astype(jnp.float32).reshape(shape)
    key_rows = key_rows.astype(jnp.float32).reshape(shape)
    value_rows = value_rows.astype(jnp.float32).reshape(shape)
    decay = jnp.exp(log_decay).reshape(shape)
    unit_keys = key_rows * lax.rsqrt(lax.optimization_barrier(jnp.sum(key_rows * key_rows, axis=-1, keepdims=True)) + KEY_EPS)
    erasing = unit_keys * learn_rate.reshape(RH, HD)

    def advance(carried, inputs):
        read_now, decay_now, key_now, value_now, unit_now, erase_now = inputs
        removed = jnp.einsum('hvk,hk->hv', carried, unit_now, precision=HIGHEST)
        carried = carried * decay_now[:, None, :] - removed[:, :, None] * erase_now[:, None, :] + value_now[:, :, None] * key_now[:, None, :]
        return (carried, jnp.einsum('hvk,hk->hv', carried, read_now, precision=HIGHEST))
    initial = jnp.zeros((RH, HD, HD), jnp.float32)
    outputs = lax.scan(advance, initial, (receptance, decay, key_rows, value_rows, unit_keys, erasing))[1]
    centered = outputs - lax.optimization_barrier(jnp.mean(outputs, axis=-1, keepdims=True))
    normal = centered * lax.rsqrt(lax.optimization_barrier(jnp.mean(centered * centered, axis=-1, keepdims=True)) + GROUP_EPS)
    return normal.reshape(TOKENS, RH * HD).astype(jnp.bfloat16)

def differential(queries, pair_keys, pair_values, mix_lambda):
    places = jnp.arange(TOKENS)
    score_scale = HD ** (-0.5)
    block_count = TOKENS // TOK_DEV

    def one_head(inputs):
        head_queries, head_keys, head_values, head_lambda = inputs
        keys_wide = head_keys.astype(jnp.float32).reshape(TOKENS, 2, HD)
        values_wide = head_values.astype(jnp.float32)
        query_blocks = head_queries.reshape(block_count, TOK_DEV, 2, HD)

        def one_block(block_inputs):
            block_queries, block_number = block_inputs
            rows_at = block_number * TOK_DEV + jnp.arange(TOK_DEV)
            scores = jnp.einsum('qmd,kmd->mqk', block_queries.astype(jnp.float32), keys_wide) * score_scale
            allowed = rows_at[:, None] >= places[None, :]
            scores = jnp.where(allowed[None], scores, -jnp.inf)
            row_max = lax.optimization_barrier(jnp.max(scores, axis=-1, keepdims=True))
            weights = jnp.exp(scores - row_max)
            row_sum = lax.optimization_barrier(jnp.sum(weights, axis=-1, keepdims=True))
            rounded = lax.optimization_barrier(weights.astype(jnp.bfloat16)).astype(jnp.float32)
            map_out = jnp.einsum('mqk,kv->mqv', rounded, values_wide) / row_sum
            head_out = map_out[0] - head_lambda * map_out[1]
            head_out = head_out * lax.rsqrt(lax.optimization_barrier(jnp.mean(head_out * head_out, axis=-1, keepdims=True)) + HEAD_EPS)
            return (head_out, (row_max + jnp.log(row_sum))[..., 0])
        outs, sums = lax.map(one_block, (query_blocks, jnp.arange(block_count)))
        return (outs.reshape(TOKENS, 2 * HD), sums.transpose(1, 0, 2).reshape(2, TOKENS))
    head_outs, log_sums = lax.map(one_head, (queries.transpose(1, 0, 2), pair_keys.transpose(1, 0, 2), pair_values.transpose(1, 0, 2), mix_lambda))
    att_mix = head_outs.transpose(1, 0, 2).reshape(TOKENS, DH * 2 * HD).astype(jnp.bfloat16)
    return (att_mix, log_sums)

def reference(hidden_in, in_gain, receptance_weight, key_weight, value_weight, decay_down, decay_up, decay_base, decay_shift, learn_rate, query_pair, key_pair, value_pair, mix_lambda, out_recurrent, out_attention, out_gain):
    normed = rms_rows(hidden_in, in_gain).astype(jnp.bfloat16)
    receptance = project(normed, receptance_weight)
    rec_keys = project(normed, key_weight)
    rec_values = project(normed, value_weight)
    low_rank = jnp.tanh(jnp.dot(normed, decay_down, preferred_element_type=jnp.float32)).astype(jnp.bfloat16)
    log_decay = -DECAY_SCALE * jax.nn.sigmoid(jnp.dot(low_rank, decay_up, preferred_element_type=jnp.float32) + decay_base) + decay_shift
    rec_mix = recurrence(receptance, rec_keys, rec_values, log_decay, learn_rate)
    queries = project(normed, query_pair).reshape(TOKENS, DH, 2 * HD)
    pair_keys = project(normed, key_pair).reshape(TOKENS, DH, 2 * HD)
    pair_values = project(normed, value_pair).reshape(TOKENS, DH, 2 * HD)
    att_mix, log_sums = differential(queries, pair_keys, pair_values, mix_lambda)
    projected = jnp.dot(rec_mix, out_recurrent, preferred_element_type=jnp.float32) + jnp.dot(att_mix, out_attention, preferred_element_type=jnp.float32)
    return (rms_rows(projected, out_gain).astype(jnp.bfloat16), log_sums)
```

```python
import functools
import math

import jax
import jax.numpy as jnp
from jax import lax
from jax.experimental import pallas as pl
from jax.experimental.pallas import tpu as pltpu
from jax.sharding import Mesh
from jax.sharding import PartitionSpec as P

F32 = jnp.float32
BF16 = jnp.bfloat16
HD = 64
NZ, NX, NY, NC = 8, 4, 4, 2
ROWS = 384
HALF = ROWS // 2
D = 2048
FEAT = 256
CHUNK = 128
SUB = 32
DECAY_SCALE = math.exp(-0.5)
NORM_EPS = 1e-06
GROUP_EPS = 0.00064
HEAD_EPS = 1e-05
KEY_EPS = 1e-06
NEGATIVE = -1e30
TINY = 1e-37
LOG2E = 1.4426950408889634
LN2 = 0.6931471805599453
MESH = pl.DeviceIdType.MESH
VMEM = pltpu.VMEM
HIGHEST = lax.Precision.HIGHEST


def dot(a, b):
    return jnp.dot(a, b, preferred_element_type=F32)


def dot_nt(a, b):
    return lax.dot_general(a, b, (((1,), (1,)), ((), ())), preferred_element_type=F32)


def split(x):
    high = x.astype(BF16)
    return high, (x - high.astype(F32)).astype(BF16)


def fine_dot(a, b):
    a_high, a_low = split(a)
    b_high, b_low = split(b)
    both = dot(jnp.concatenate([a_high, a_low], 1), jnp.concatenate([b_high, b_high], 0))
    return both + dot(a_high, b_low)


def fine_dot_nt(a, b):
    a_high, a_low = split(a)
    b_high, b_low = split(b)
    both = dot_nt(jnp.concatenate([a_high, a_low], 1), jnp.concatenate([b_high, b_high], 1))
    return both + dot_nt(a_high, b_low)


def coarse_dot(a, b):
    return dot(a.astype(BF16), b.astype(BF16))


def remote(src, dst, send_sem, recv_sem, where):
    return pltpu.make_async_remote_copy(
        src_ref=src,
        dst_ref=dst,
        send_sem=send_sem,
        recv_sem=recv_sem,
        device_id=where,
        device_id_type=MESH,
    )


def greet(places):
    barrier = pltpu.get_barrier_semaphore()
    for place in places:
        pl.semaphore_signal(barrier, inc=1, device_id=place, device_id_type=MESH)
    pl.semaphore_wait(barrier, len(places))


def gather_project(
    hid_ref,
    gain_ref,
    up_ref,
    base_ref,
    shift_ref,
    *rest,
):
    weights = rest[:7]
    q_ref, k_ref, vt_ref, r_ref, rk_ref, rv_ref, ld_ref = rest[7:14]
    hbuf, wbuf, acc, sumsq, wsem, ssem, rsem = rest[14:]
    y = lax.axis_index("y")
    c = lax.axis_index("c")
    other = 1 - c
    up, down, across = lax.rem(y + 1, NY), lax.rem(y + 3, NY), lax.rem(y + 2, NY)
    loads = []
    for n, w in enumerate(weights):
        load = pltpu.make_async_copy(w, wbuf.at[:, pl.ds(n * 128, 128)], wsem.at[n])
        load.start()
        loads.append(load)
    to_up, to_down, to_other = {"y": up}, {"y": down}, {"c": other}
    greet([to_up, to_down, to_other])

    own = y * 2 + c

    def send(n, src, dst, where):
        copy = remote(src, dst, ssem.at[n], rsem.at[n], where)
        copy.start()
        return copy

    first, second = pl.ds(0, HALF), pl.ds(HALF, HALF)
    copies = [None] * 9
    copies[0] = send(0, hid_ref, hbuf.at[own], to_up)
    copies[1] = send(1, hid_ref, hbuf.at[own], to_down)
    copies[2] = send(2, hid_ref, hbuf.at[own], to_other)
    for load in loads:
        load.wait()

    def add(block, number, fresh=False):
        w = wbuf[pl.ds(pl.multiple_of(number * FEAT, FEAT), FEAT), :]
        gain = gain_ref[pl.ds(number, 1), :]

        @pl.loop(0, ROWS // 128)
        def _(t):
            rows = pl.ds(pl.multiple_of(t * 128, 128), 128)
            h = block[rows, :].astype(F32)
            squares = h[:, :128] * h[:, :128] + h[:, 128:] * h[:, 128:]
            product = dot((h * gain).astype(BF16), w)
            if fresh:
                sumsq[rows, :] = squares
                acc[rows, :] = product
            else:
                sumsq[rows, :] += squares
                acc[rows, :] += product

    add(hid_ref, own, True)
    copies[2].wait_recv()
    add(hbuf.at[y * 2 + other], y * 2 + other)
    copies[0].wait_recv()
    below = hbuf.at[down * 2 + c]
    copies[3] = send(3, below.at[first], below.at[first], to_up)
    copies[4] = send(4, below, below, to_other)
    copies[1].wait_recv()
    above = hbuf.at[up * 2 + c]
    copies[5] = send(5, above.at[second], above.at[second], to_down)
    copies[6] = send(6, above, above, to_other)
    add(below, down * 2 + c)
    add(above, up * 2 + c)
    copies[4].wait_recv()
    add(hbuf.at[down * 2 + other], down * 2 + other)
    copies[6].wait_recv()
    add(hbuf.at[up * 2 + other], up * 2 + other)
    far = hbuf.at[across * 2 + c]
    copies[3].wait_recv()
    copies[7] = send(7, far.at[first], far.at[first], to_other)
    copies[5].wait_recv()
    copies[8] = send(8, far.at[second], far.at[second], to_other)
    add(far, across * 2 + c)
    copies[7].wait_recv()
    copies[8].wait_recv()
    add(hbuf.at[across * 2 + other], across * 2 + other)

    @pl.loop(0, ROWS // 128)
    def _(t):
        rows = pl.ds(pl.multiple_of(t * 128, 128), 128)
        total = jnp.sum(sumsq[rows, :], axis=1, keepdims=True)
        scale = lax.rsqrt(total * (1.0 / D) + NORM_EPS)
        r_ref[rows, :] = (acc[rows, 0:128] * scale).astype(BF16)
        rk_ref[rows, :] = (acc[rows, 128:256] * scale).astype(BF16)
        rv_ref[rows, :] = (acc[rows, 256:384] * scale).astype(BF16)
        low = jnp.tanh(acc[rows, 384:512] * scale).astype(BF16)
        gate = dot(low, up_ref[...]) + base_ref[...]
        ld_ref[rows, :] = -DECAY_SCALE * jax.nn.sigmoid(gate) + shift_ref[rows, :]
        q_ref[rows, :] = (acc[rows, 512:640] * (scale * (LOG2E * HD**-0.5))).astype(BF16)
        k_ref[rows, :] = (acc[rows, 640:768] * scale).astype(BF16)

    total = jnp.sum(sumsq[...], axis=1, keepdims=True)
    scale = lax.rsqrt(total * (1.0 / D) + NORM_EPS)
    vt_ref[...] = jnp.transpose(acc[:, 768:896] * scale).astype(BF16)
    for copy in copies:
        copy.wait_send()


def run_gather_project(hid, gain, up, base, shift, weights):
    whole = pl.BlockSpec(memory_space=VMEM)
    far = pl.BlockSpec(memory_space=pl.ANY)
    rows = jax.ShapeDtypeStruct((ROWS, 128), BF16)
    return pl.pallas_call(
        gather_project,
        out_shape=(
            rows,
            rows,
            jax.ShapeDtypeStruct((128, ROWS), BF16),
            rows,
            rows,
            rows,
            jax.ShapeDtypeStruct((ROWS, 128), F32),
        ),
        in_specs=[whole] * 5 + [far] * 7,
        out_specs=(whole,) * 7,
        scratch_shapes=[
            VMEM((NY * NC, ROWS, FEAT), BF16),
            VMEM((D, 896), BF16),
            VMEM((ROWS, 896), F32),
            VMEM((ROWS, 128), F32),
            pltpu.SemaphoreType.DMA((7,)),
            pltpu.SemaphoreType.DMA((9,)),
            pltpu.SemaphoreType.DMA((9,)),
        ],
        compiler_params=pltpu.CompilerParams(
            collective_id=0, has_side_effects=True, vmem_limit_bytes=40 * 2**20
        ),
        name="gather_project",
    )(hid, gain, up, base, shift, *weights)


def iota(shape, dim):
    return lax.broadcasted_iota(jnp.int32, shape, dim)


def by_head(x):
    first = lax.rem(iota(x.shape, 1), 128) < HD
    zero = jnp.zeros_like(x)
    return jnp.concatenate([jnp.where(first, x, zero), jnp.where(first, zero, x)], 0)


def same_head(shape):
    return (iota(shape, 0) < HD) == (lax.rem(iota(shape, 1), 128) < HD)


def inverse(lower):
    row, col = iota((CHUNK, CHUNK), 0), iota((CHUNK, CHUNK), 1)
    found = None
    size = 1
    while size < CHUNK:
        here = (
            (lax.div(row, 2 * size) == lax.div(col, 2 * size))
            & (lax.rem(row, 2 * size) >= size)
            & (lax.rem(col, 2 * size) < size)
        )
        part = jnp.where(here, lower, 0.0)
        if found is None:
            found = jnp.where(row == col, 1.0, part)
        else:
            found = found + coarse_dot(coarse_dot(found, part), found)
        size *= 2
    return found


def chunk_terms(r, k, v, w, rate):
    row, col = iota((CHUNK, CHUNK), 0), iota((CHUNK, CHUNK), 1)
    causal = (row >= col).astype(F32)
    running = jnp.dot(causal, w, precision=HIGHEST, preferred_element_type=F32)
    before = running - w
    ending = running[CHUNK - 1 :, :]
    first = col < HD
    square = k * k
    norm_one = jnp.sum(jnp.where(first, square, 0.0), axis=1, keepdims=True)
    norm_two = jnp.sum(jnp.where(first, 0.0, square), axis=1, keepdims=True)
    unit = k * jnp.where(first, lax.rsqrt(norm_one + KEY_EPS), lax.rsqrt(norm_two + KEY_EPS))
    erasing = unit * rate
    against = -unit
    pieces = []
    for i in range(CHUNK // SUB):
        at = slice(i * SUB, (i + 1) * SUB)
        start = running[i * SUB - 1 : i * SUB, :] if i else jnp.zeros_like(ending)
        left = jnp.concatenate(
            [
                against[at] * jnp.exp(before[at] - start),
                r[at] * jnp.exp(running[at] - start),
            ],
            0,
        )
        growth = jnp.exp(jnp.where(row < (i + 1) * SUB, start - running, -100.0))
        right = jnp.concatenate([erasing * growth, k * growth], 0)
        pieces.append(fine_dot_nt(by_head(left), right))

    def matrix(head, read, keys, keep):
        at = head * 2 * SUB + read * SUB
        whole = jnp.concatenate(
            [p[at : at + SUB, keys * CHUNK : (keys + 1) * CHUNK] for p in pieces], 0
        )
        return jnp.where(keep, whole, 0.0)

    strict, causal = row > col, row >= col
    inverses = [inverse(matrix(h, 0, 0, strict)) for h in range(2)]
    carry = [matrix(h, 0, 1, strict).astype(BF16) for h in range(2)]
    read_erase = [matrix(h, 1, 0, causal).astype(BF16) for h in range(2)]
    read_keys = [matrix(h, 1, 1, causal).astype(BF16) for h in range(2)]
    values = by_head(v)
    carried = dot(jnp.concatenate(carry, 1), values)
    right_side = by_head(jnp.concatenate([against * jnp.exp(before), carried], 1))
    solved = fine_dot(jnp.concatenate(inverses, 1), right_side)
    seen = dot(jnp.concatenate(read_erase, 1), by_head(solved.astype(BF16)))
    read_state = r * jnp.exp(running) + seen[:, :128]
    local = seen[:, 128:] + dot(jnp.concatenate(read_keys, 1), values)
    to_end = jnp.exp(ending - running)
    left = jnp.concatenate(
        [jnp.transpose(erasing * to_end), jnp.transpose(k * to_end)], 1
    )
    none = jnp.zeros((CHUNK, 128), F32)
    right = jnp.concatenate(
        [solved, jnp.concatenate([none, v.astype(F32)], 1)], 0
    )
    step = jnp.where(same_head((128, 256)), fine_dot(left, right), 0.0)
    wide_row, wide_col = iota((128, 256), 0), iota((128, 256), 1)
    decayed = jnp.concatenate([jnp.broadcast_to(jnp.exp(ending), (128, 128)), none], 1)
    step = step + jnp.where(wide_row == wide_col, decayed, 0.0)
    return read_state, local, step


def compose(later, earlier):
    out = fine_dot(later[:, :128], earlier)
    none = jnp.zeros((128, 128), F32)
    return out + jnp.concatenate([none, later[:, 128:]], 1)


def packed(step):
    return step[:HD] + step[HD:]


def unpacked(step):
    both = jnp.concatenate([step, step], 0)
    return jnp.where(same_head((128, 256)), both, 0.0)


def packed_identity():
    row, col = iota((HD, 256), 0), iota((HD, 256), 1)
    return jnp.where((col < 128) & (lax.rem(col, HD) == row), 1.0, 0.0)


def mixers(
    lam_ref,
    q_ref,
    k_ref,
    vt_ref,
    r_ref,
    rk_ref,
    rv_ref,
    ld_ref,
    rate_ref,
    mix_ref,
    sums_ref,
    kbuf,
    vbuf,
    qbuf,
    qwide,
    acc,
    top,
    low,
    osend,
    orecv,
    stsend,
    strecv,
    gxsend,
    gxbuf,
    gzsend,
    gzbuf,
    reads,
    local,
    ssem,
    rsem,
):
    z = lax.axis_index("z")
    x = lax.axis_index("x")
    z_up, z_down = {"z": lax.rem(z + 1, NZ)}, {"z": lax.rem(z + NZ - 1, NZ)}
    z_others = [{"z": lax.rem(z + n, NZ)} for n in range(1, NZ)]
    x_others = [lax.rem(x + n, NX) for n in range(1, NX)]
    greet(z_others + [{"x": n} for n in x_others])

    copies = []

    def send(src, dst, where):
        n = len(copies)
        copy = remote(src, dst, ssem.at[n], rsem.at[n], where)
        copy.start()
        copies.append(copy)
        return copy

    def forward(k_src, v_src, slot, where):
        return (
            send(k_src, kbuf.at[slot], where),
            send(v_src, vbuf.at[slot], where),
        )

    def arrived(pair):
        for copy in pair:
            copy.wait_recv()

    up1 = forward(k_ref, vt_ref, 0, z_up)
    down1 = forward(k_ref, vt_ref, 3, z_down)
    q_copies = [send(q_ref, qbuf.at[x], {"x": n}) for n in x_others]

    rate = rate_ref[...]
    so_far = None
    for n in range(ROWS // CHUNK):
        at = slice(n * CHUNK, (n + 1) * CHUNK)
        read_state, here, step = chunk_terms(
            r_ref[at, :].astype(F32),
            rk_ref[at, :].astype(F32),
            rv_ref[at, :],
            ld_ref[at, :],
            rate,
        )
        if so_far is None:
            reads[at, :] = read_state
            local[at, :] = here
            so_far = step
        else:
            seen = fine_dot(read_state, so_far)
            reads[at, :] = seen[:, :128]
            local[at, :] = here + seen[:, 128:]
            so_far = compose(step, so_far)
    gxsend[...] = packed(so_far)
    gxbuf[x] = packed(so_far)
    gx_copies = [send(gxsend, gxbuf.at[x], {"x": n}) for n in x_others]

    arrived(up1)
    up2 = forward(kbuf.at[0], vbuf.at[0], 1, z_up)
    arrived(down1)
    down2 = forward(kbuf.at[3], vbuf.at[3], 4, z_down)

    top[...] = jnp.full((NX, 8, 2 * ROWS), NEGATIVE, F32)
    low[...] = jnp.zeros((NX, 8, 2 * ROWS), F32)
    acc[...] = jnp.zeros((NX, 128, 2 * ROWS), F32)
    qbuf[x] = q_ref[...]
    for copy in q_copies:
        copy.wait_recv()
    for j in range(NX):
        qwide[j] = by_head(qbuf[j])

    def attend_one(k_block, v_block, j, masked):
        for t in range(3):
            cols = slice(t * 256, (t + 1) * 256)
            scores = dot_nt(k_block[...], qwide[j, cols, :])
            if masked:
                key_at = iota((ROWS, 256), 0)
                query_at = lax.rem(iota((ROWS, 256), 1) + t * 256, ROWS)
                scores = jnp.where(query_at >= key_at, scores, NEGATIVE)
            old = top[j, 0:1, cols]
            new = jnp.maximum(old, jnp.max(scores, axis=0, keepdims=True))
            weights = jnp.exp2(scores - new)
            rescale = jnp.exp2(old - new)
            top[j, 0:1, cols] = new
            low[j, 0:1, cols] = low[j, 0:1, cols] * rescale + jnp.sum(
                weights, axis=0, keepdims=True
            )
            acc[j, :, cols] = acc[j, :, cols] * rescale + dot(
                v_block[...], weights.astype(BF16)
            )

    def attend(slot, needed):
        @pl.when(needed)
        def _():
            @pl.loop(0, NX)
            def _(j):
                attend_one(kbuf.at[slot], vbuf.at[slot], j, False)

    attend_one(k_ref, vt_ref, x, True)

    @pl.loop(0, NX)
    def _(j):
        @pl.when(j > x)
        def _():
            attend_one(k_ref, vt_ref, j, False)

    attend(0, z >= 1)
    attend(3, z >= NZ - 1)

    for copy in gx_copies:
        copy.wait_recv()
    none = jnp.zeros((128, 128), F32)
    identity = jnp.where(iota((128, 256), 0) == iota((128, 256), 1), 1.0, 0.0)
    before_x = identity
    total = unpacked(gxbuf[0])
    for n in range(1, NX):
        before_x = jnp.where(x == n, total, before_x)
        total = compose(unpacked(gxbuf[n]), total)
    share = (packed(total) - packed_identity()).astype(BF16)
    gzsend[...] = share
    gzbuf[z] = share
    gz_copies = [send(gzsend, gzbuf.at[z], place) for place in z_others]

    arrived(up2)
    up3 = forward(kbuf.at[1], vbuf.at[1], 2, z_up)
    arrived(down2)
    down3 = forward(kbuf.at[4], vbuf.at[4], 5, z_down)
    attend(1, z >= 2)
    attend(4, z >= NZ - 2)

    arrived(up3)
    key_one, key_two = pl.ds(0, HALF), pl.ds(HALF, HALF)
    value_one, value_two = pl.ds(0, HD), pl.ds(HD, HD)
    up4 = (
        send(kbuf.at[2, key_one], kbuf.at[6, key_one], z_up),
        send(vbuf.at[2, value_one], vbuf.at[6, value_one], z_up),
    )
    arrived(down3)
    down4 = (
        send(kbuf.at[5, key_two], kbuf.at[6, key_two], z_down),
        send(vbuf.at[5, value_two], vbuf.at[6, value_two], z_down),
    )
    attend(2, z >= 3)
    attend(5, z >= NZ - 3)

    for copy in gz_copies:
        copy.wait_recv()
    state = none
    for n in range(NZ - 1):
        step = unpacked(gzbuf[n].astype(F32) + packed_identity())
        after = fine_dot(step[:, :128], state) + step[:, 128:]
        state = jnp.where(n < z, after, state)
    state = fine_dot(before_x[:, :128], state) + before_x[:, 128:]
    recurrent = local[...] + fine_dot(reads[...], state)
    first = iota((ROWS, 128), 1) < HD

    def head_mean(values):
        one = jnp.sum(jnp.where(first, values, 0.0), axis=1, keepdims=True)
        two = jnp.sum(jnp.where(first, 0.0, values), axis=1, keepdims=True)
        return jnp.where(first, one, two) * (1.0 / HD)

    centered = recurrent - head_mean(recurrent)
    normal = centered * lax.rsqrt(head_mean(centered * centered) + GROUP_EPS)
    mix_ref[:, 0:128] = normal.astype(BF16)

    arrived(up4)
    arrived(down4)
    attend(6, z >= 4)

    def partial_out(j):
        total = jnp.maximum(low[j, 0:1, :], TINY)
        return acc[j] * (1.0 / total), top[j, 0:1, :] + jnp.log2(total)

    o_copies = []
    for n in (1, 0, 2):
        j = x_others[n]
        out, level = partial_out(j)
        osend[n] = out.astype(BF16)
        stsend[n] = jnp.broadcast_to(level, (8, 2 * ROWS))
        o_copies.append(send(osend.at[n], orecv.at[n], {"x": j}))
        o_copies.append(send(stsend.at[n], strecv.at[n], {"x": j}))
    own_out, own_level = partial_out(x)
    for copy in o_copies:
        copy.wait_recv()
    levels = [own_level] + [strecv[n, 0:1, :] for n in range(3)]
    highest = functools.reduce(jnp.maximum, levels)
    shares = [jnp.exp2(level - highest) for level in levels]
    share_sum = sum(shares)
    map_out = own_out * (shares[0] / share_sum)
    for n in range(3):
        map_out = map_out + orecv[n].astype(F32) * (shares[n + 1] / share_sum)
    sums = (highest + jnp.log2(share_sum)) * LN2
    sums_ref[0:1, :] = sums[:, :ROWS]
    sums_ref[1:2, :] = sums[:, ROWS:]
    head_out = map_out[:, :ROWS] - lam_ref[0] * map_out[:, ROWS:]
    head_out = head_out * lax.rsqrt(
        jnp.mean(head_out * head_out, axis=0, keepdims=True) + HEAD_EPS
    )
    mix_ref[:, 128:256] = jnp.transpose(head_out).astype(BF16)
    for copy in copies:
        copy.wait_send()


def run_mixers(lam, q, k, vt, r, rk, rv, ld, rate):
    whole = pl.BlockSpec(memory_space=VMEM)
    count = 16 + 3 + 3 + 7 + 6
    return pl.pallas_call(
        mixers,
        out_shape=(
            jax.ShapeDtypeStruct((ROWS, 256), BF16),
            jax.ShapeDtypeStruct((2, ROWS), F32),
        ),
        in_specs=[pl.BlockSpec(memory_space=pltpu.SMEM)] + [whole] * 8,
        out_specs=(whole, whole),
        scratch_shapes=[
            VMEM((7, ROWS, 128), BF16),
            VMEM((7, 128, ROWS), BF16),
            VMEM((NX, ROWS, 128), BF16),
            VMEM((NX, 2 * ROWS, 128), BF16),
            VMEM((NX, 128, 2 * ROWS), F32),
            VMEM((NX, 8, 2 * ROWS), F32),
            VMEM((NX, 8, 2 * ROWS), F32),
            VMEM((3, 128, 2 * ROWS), BF16),
            VMEM((3, 128, 2 * ROWS), BF16),
            VMEM((3, 8, 2 * ROWS), F32),
            VMEM((3, 8, 2 * ROWS), F32),
            VMEM((HD, 256), F32),
            VMEM((NX, HD, 256), F32),
            VMEM((HD, 256), BF16),
            VMEM((NZ, HD, 256), BF16),
            VMEM((ROWS, 128), F32),
            VMEM((ROWS, 128), F32),
            pltpu.SemaphoreType.DMA((count,)),
            pltpu.SemaphoreType.DMA((count,)),
        ],
        compiler_params=pltpu.CompilerParams(
            collective_id=1, has_side_effects=True, vmem_limit_bytes=48 * 2**20
        ),
        name="mixers",
    )(lam, q, k, vt, r, rk, rv, ld, rate)


def project_sum(
    mix_ref,
    gain_ref,
    wr_ref,
    wa_ref,
    out_ref,
    wbuf,
    psend,
    precv,
    pair,
    hsend,
    hrecv,
    wsem,
    ssem,
    rsem,
):
    y = lax.axis_index("y")
    c = lax.axis_index("c")
    other = 1 - c
    up, down, across = lax.rem(y + 1, NY), lax.rem(y + 3, NY), lax.rem(y + 2, NY)
    loads = [
        pltpu.make_async_copy(wr_ref, wbuf.at[pl.ds(0, 128)], wsem.at[0]),
        pltpu.make_async_copy(wa_ref, wbuf.at[pl.ds(128, 128)], wsem.at[1]),
    ]
    for load in loads:
        load.start()
    to_up, to_down, to_other = {"y": up}, {"y": down}, {"c": other}
    greet([to_up, to_down, to_other])
    share = ROWS // (NY * NC)
    order = [across, up, down, y]

    def rows_for(core):
        return jnp.concatenate(
            [
                mix_ref[pl.ds(pl.multiple_of((n * 2 + core) * share, share), share), :]
                for n in order
            ],
            0,
        )

    for load in loads:
        load.wait()

    theirs = rows_for(other)
    ours = rows_for(c)
    for t in range(8):
        cols = slice(t * 256, (t + 1) * 256)
        psend[:, cols] = dot(theirs, wbuf[:, cols]).astype(BF16)
    copies = []

    def send(src, dst, where):
        n = len(copies)
        copy = remote(src, dst, ssem.at[n], rsem.at[n], where)
        copy.start()
        copies.append(copy)
        return copy

    pairs = [
        send(psend.at[pl.ds(n * share, share)], precv.at[pl.ds(n * share, share)], to_other)
        for n in range(4)
    ]
    for t in range(8):
        cols = slice(t * 256, (t + 1) * 256)
        pair[:, cols] = dot(ours, wbuf[:, cols])
    one, two = slice(0, D // 2), slice(D // 2, D)

    def summed(n, half):
        at = slice(n * share, (n + 1) * share)
        return pair[at, half] + precv[at, half].astype(F32)

    pairs[0].wait_recv()
    hsend[0] = summed(0, one).astype(BF16)
    relay_up = send(hsend.at[0], hrecv.at[0], to_up)
    hsend[1] = summed(0, two).astype(BF16)
    relay_down = send(hsend.at[1], hrecv.at[1], to_down)
    pairs[1].wait_recv()
    hsend[2] = summed(1, two).astype(BF16)
    plain_up = send(hsend.at[2], hrecv.at[2], to_up)
    pairs[2].wait_recv()
    hsend[3] = summed(2, one).astype(BF16)
    plain_down = send(hsend.at[3], hrecv.at[3], to_down)
    relay_up.wait_recv()
    hsend[4] = (summed(1, one) + hrecv[0].astype(F32)).astype(BF16)
    merged_up = send(hsend.at[4], hrecv.at[4], to_up)
    relay_down.wait_recv()
    hsend[5] = (summed(2, two) + hrecv[1].astype(F32)).astype(BF16)
    merged_down = send(hsend.at[5], hrecv.at[5], to_down)
    pairs[3].wait_recv()
    plain_up.wait_recv()
    plain_down.wait_recv()
    left = summed(3, one) + hrecv[3].astype(F32)
    right = summed(3, two) + hrecv[2].astype(F32)
    merged_up.wait_recv()
    merged_down.wait_recv()
    left = left + hrecv[4].astype(F32)
    right = right + hrecv[5].astype(F32)
    total = jnp.sum(left * left, axis=1, keepdims=True) + jnp.sum(
        right * right, axis=1, keepdims=True
    )
    scale = lax.rsqrt(total * (1.0 / D) + NORM_EPS)
    out_ref[:, one] = (left * scale * gain_ref[:, one]).astype(BF16)
    out_ref[:, two] = (right * scale * gain_ref[:, two]).astype(BF16)
    for copy in copies:
        copy.wait_send()


def run_project_sum(mix, gain, wr, wa):
    whole = pl.BlockSpec(memory_space=VMEM)
    far = pl.BlockSpec(memory_space=pl.ANY)
    share = ROWS // (NY * NC)
    return pl.pallas_call(
        project_sum,
        out_shape=jax.ShapeDtypeStruct((share, D), BF16),
        in_specs=[whole, whole, far, far],
        out_specs=whole,
        scratch_shapes=[
            VMEM((256, D), BF16),
            VMEM((4 * share, D), BF16),
            VMEM((4 * share, D), BF16),
            VMEM((4 * share, D), F32),
            VMEM((6, share, D // 2), BF16),
            VMEM((6, share, D // 2), BF16),
            pltpu.SemaphoreType.DMA((2,)),
            pltpu.SemaphoreType.DMA((10,)),
            pltpu.SemaphoreType.DMA((10,)),
        ],
        compiler_params=pltpu.CompilerParams(
            collective_id=2, has_side_effects=True, vmem_limit_bytes=40 * 2**20
        ),
        name="project_sum",
    )(mix, gain, wr, wa)


def per_device(
    hidden_in,
    in_gain,
    receptance_weight,
    key_weight,
    value_weight,
    decay_down,
    decay_up,
    decay_base,
    decay_shift,
    learn_rate,
    query_pair,
    key_pair,
    value_pair,
    mix_lambda,
    out_recurrent,
    out_attention,
    out_gain,
):
    q, k, vt, r, rk, rv, ld = run_gather_project(
        hidden_in,
        in_gain.reshape(NY * NC, FEAT),
        decay_up,
        decay_base.reshape(1, 128),
        decay_shift,
        (
            receptance_weight,
            key_weight,
            value_weight,
            decay_down,
            query_pair.reshape(D, 128),
            key_pair.reshape(D, 128),
            value_pair.reshape(D, 128),
        ),
    )
    mix, sums = run_mixers(
        mix_lambda, q, k, vt, r, rk, rv, ld, learn_rate.reshape(1, 128)
    )
    layer_out = run_project_sum(mix, out_gain.reshape(1, D), out_recurrent, out_attention)
    return layer_out, sums.reshape(1, 2, ROWS)


def solution(mesh):
    split_mesh = Mesh(mesh.devices.reshape(NZ, NX, NY, NC), ("z", "x", "y", "c"))
    sp, tp = ("z", "x"), ("y", "c")
    placed = (
        P(sp, tp),
        P(),
        P(None, tp),
        P(None, tp),
        P(None, tp),
        P(),
        P(None, tp),
        P(tp),
        P(sp, tp),
        P(tp),
        P(None, tp, None),
        P(None, tp, None),
        P(None, tp, None),
        P(tp),
        P(tp, None),
        P(tp, None),
        P(),
    )
    return jax.shard_map(
        per_device,
        mesh=split_mesh,
        in_specs=placed,
        out_specs=(P((*sp, *tp), None), P(tp, None, sp)),
        check_vma=False,
    )
```

```python
import functools
import math

import jax
import jax.numpy as jnp
from jax import lax
from jax.experimental import pallas as pl
from jax.experimental.pallas import tpu as pltpu
from jax.sharding import Mesh
from jax.sharding import PartitionSpec as P

F32 = jnp.float32
BF16 = jnp.bfloat16
HD = 64
NZ, NX, NY, NC = 8, 4, 4, 2
ROWS = 384
HALF = ROWS // 2
D = 2048
FEAT = 256
CHUNK = 128
SUB = 32
DECAY_SCALE = math.exp(-0.5)
NORM_EPS = 1e-06
GROUP_EPS = 0.00064
HEAD_EPS = 1e-05
KEY_EPS = 1e-06
NEGATIVE = -1e30
TINY = 1e-37
LOG2E = 1.4426950408889634
LN2 = 0.6931471805599453
MESH = pl.DeviceIdType.MESH
VMEM = pltpu.VMEM
HIGHEST = lax.Precision.HIGHEST


def dot(a, b):
    return jnp.dot(a, b, preferred_element_type=F32)


def dot_nt(a, b):
    return lax.dot_general(a, b, (((1,), (1,)), ((), ())), preferred_element_type=F32)


def split(x):
    high = x.astype(BF16)
    return high, (x - high.astype(F32)).astype(BF16)


def fine_dot(a, b):
    a_high, a_low = split(a)
    b_high, b_low = split(b)
    both = dot(jnp.concatenate([a_high, a_low], 1), jnp.concatenate([b_high, b_high], 0))
    return both + dot(a_high, b_low)


def fine_dot_nt(a, b):
    a_high, a_low = split(a)
    b_high, b_low = split(b)
    both = dot_nt(jnp.concatenate([a_high, a_low], 1), jnp.concatenate([b_high, b_high], 1))
    return both + dot_nt(a_high, b_low)


def coarse_dot(a, b):
    return dot(a.astype(BF16), b.astype(BF16))


def remote(src, dst, send_sem, recv_sem, where):
    return pltpu.make_async_remote_copy(
        src_ref=src,
        dst_ref=dst,
        send_sem=send_sem,
        recv_sem=recv_sem,
        device_id=where,
        device_id_type=MESH,
    )


def greet(places):
    barrier = pltpu.get_barrier_semaphore()
    for place in places:
        pl.semaphore_signal(barrier, inc=1, device_id=place, device_id_type=MESH)
    pl.semaphore_wait(barrier, len(places))


def iota(shape, dim):
    return lax.broadcasted_iota(jnp.int32, shape, dim)


def by_head(x):
    first = lax.rem(iota(x.shape, 1), 128) < HD
    zero = jnp.zeros_like(x)
    return jnp.concatenate([jnp.where(first, x, zero), jnp.where(first, zero, x)], 0)


def same_head(shape):
    return (iota(shape, 0) < HD) == (lax.rem(iota(shape, 1), 128) < HD)


def inverse(lower):
    row, col = iota((CHUNK, CHUNK), 0), iota((CHUNK, CHUNK), 1)
    found = None
    size = 1
    while size < CHUNK:
        here = (
            (lax.div(row, 2 * size) == lax.div(col, 2 * size))
            & (lax.rem(row, 2 * size) >= size)
            & (lax.rem(col, 2 * size) < size)
        )
        part = jnp.where(here, lower, 0.0)
        if found is None:
            found = jnp.where(row == col, 1.0, part)
        else:
            found = found + coarse_dot(coarse_dot(found, part), found)
        size *= 2
    return found


def chunk_terms(r, k, v, w, rate):
    row, col = iota((CHUNK, CHUNK), 0), iota((CHUNK, CHUNK), 1)
    causal = (row >= col).astype(F32)
    running = jnp.dot(causal, w, precision=HIGHEST, preferred_element_type=F32)
    before = running - w
    ending = running[CHUNK - 1 :, :]
    first = col < HD
    square = k * k
    norm_one = jnp.sum(jnp.where(first, square, 0.0), axis=1, keepdims=True)
    norm_two = jnp.sum(jnp.where(first, 0.0, square), axis=1, keepdims=True)
    unit = k * jnp.where(first, lax.rsqrt(norm_one + KEY_EPS), lax.rsqrt(norm_two + KEY_EPS))
    erasing = unit * rate
    against = -unit
    pieces = []
    for i in range(CHUNK // SUB):
        at = slice(i * SUB, (i + 1) * SUB)
        start = running[i * SUB - 1 : i * SUB, :] if i else jnp.zeros_like(ending)
        left = jnp.concatenate(
            [
                against[at] * jnp.exp(before[at] - start),
                r[at] * jnp.exp(running[at] - start),
            ],
            0,
        )
        growth = jnp.exp(jnp.where(row < (i + 1) * SUB, start - running, -100.0))
        right = jnp.concatenate([erasing * growth, k * growth], 0)
        pieces.append(fine_dot_nt(by_head(left), right))

    def matrix(head, read, keys, keep):
        at = head * 2 * SUB + read * SUB
        whole = jnp.concatenate(
            [p[at : at + SUB, keys * CHUNK : (keys + 1) * CHUNK] for p in pieces], 0
        )
        return jnp.where(keep, whole, 0.0)

    strict, causal = row > col, row >= col
    inverses = [inverse(matrix(h, 0, 0, strict)) for h in range(2)]
    carry = [matrix(h, 0, 1, strict).astype(BF16) for h in range(2)]
    read_erase = [matrix(h, 1, 0, causal).astype(BF16) for h in range(2)]
    read_keys = [matrix(h, 1, 1, causal).astype(BF16) for h in range(2)]
    values = by_head(v)
    carried = dot(jnp.concatenate(carry, 1), values)
    right_side = by_head(jnp.concatenate([against * jnp.exp(before), carried], 1))
    solved = fine_dot(jnp.concatenate(inverses, 1), right_side)
    seen = dot(jnp.concatenate(read_erase, 1), by_head(solved.astype(BF16)))
    read_state = r * jnp.exp(running) + seen[:, :128]
    local = seen[:, 128:] + dot(jnp.concatenate(read_keys, 1), values)
    to_end = jnp.exp(ending - running)
    left = jnp.concatenate(
        [jnp.transpose(erasing * to_end), jnp.transpose(k * to_end)], 1
    )
    none = jnp.zeros((CHUNK, 128), F32)
    right = jnp.concatenate(
        [solved, jnp.concatenate([none, v.astype(F32)], 1)], 0
    )
    step = jnp.where(same_head((128, 256)), fine_dot(left, right), 0.0)
    wide_row, wide_col = iota((128, 256), 0), iota((128, 256), 1)
    decayed = jnp.concatenate([jnp.broadcast_to(jnp.exp(ending), (128, 128)), none], 1)
    step = step + jnp.where(wide_row == wide_col, decayed, 0.0)
    return read_state, local, step


def compose(later, earlier):
    out = fine_dot(later[:, :128], earlier)
    none = jnp.zeros((128, 128), F32)
    return out + jnp.concatenate([none, later[:, 128:]], 1)


def packed(step):
    return step[:HD] + step[HD:]


def unpacked(step):
    both = jnp.concatenate([step, step], 0)
    return jnp.where(same_head((128, 256)), both, 0.0)


def packed_identity():
    row, col = iota((HD, 256), 0), iota((HD, 256), 1)
    return jnp.where((col < 128) & (lax.rem(col, HD) == row), 1.0, 0.0)


class Courier:
    def __init__(self, ssem, rsem):
        self.ssem, self.rsem, self.copies = ssem, rsem, []

    def send(self, src, dst, where):
        n = len(self.copies)
        copy = remote(src, dst, self.ssem.at[n], self.rsem.at[n], where)
        copy.start()
        self.copies.append(copy)
        return copy


def load_all(places, sems, first):
    loads = []
    for n, (src, dst) in enumerate(places):
        load = pltpu.make_async_copy(src, dst, sems.at[first + n])
        load.start()
        loads.append(load)
    return loads


def layer(
    lam_ref,
    hid_hbm,
    gain_hbm,
    up_hbm,
    base_hbm,
    shift_hbm,
    rate_hbm,
    wr_hbm,
    wa_hbm,
    out_gain_hbm,
    *rest,
):
    weights = rest[:7]
    out_ref, sums_ref = rest[7:9]
    (
        hbuf,
        wbuf,
        proj,
        sumsq,
        gain_ref,
        up_ref,
        base_ref,
        shift_ref,
        rate_ref,
        out_w,
        out_gain_ref,
        q_ref,
        k_ref,
        vt_ref,
        r_ref,
        rk_ref,
        rv_ref,
        ld_ref,
        kbuf,
        vbuf,
        qbuf,
        qwide,
        acc,
        top,
        low,
        osend,
        orecv,
        stsend,
        strecv,
        gxsend,
        gxbuf,
        gzsend,
        gzbuf,
        reads,
        local,
        mix_ref,
        psend,
        precv,
        pair,
        hsend,
        hrecv,
        wsem,
        ssem,
        rsem,
    ) = rest[9:]
    z = lax.axis_index("z")
    x = lax.axis_index("x")
    y = lax.axis_index("y")
    c = lax.axis_index("c")
    other = 1 - c
    up, down, across = lax.rem(y + 1, NY), lax.rem(y + 3, NY), lax.rem(y + 2, NY)
    own = y * 2 + c
    loads = load_all([(hid_hbm, hbuf.at[own])], wsem, 0)
    places = [(w, wbuf.at[:, pl.ds(n * 128, 128)]) for n, w in enumerate(weights)]
    places += [
        (gain_hbm, gain_ref),
        (up_hbm, up_ref),
        (base_hbm, base_ref),
        (shift_hbm, shift_ref),
        (rate_hbm, rate_ref),
        (wr_hbm, out_w.at[pl.ds(0, 128)]),
        (wa_hbm, out_w.at[pl.ds(128, 128)]),
        (out_gain_hbm, out_gain_ref),
    ]
    loads += load_all(places, wsem, 1)
    to_up, to_down, to_other = {"y": up}, {"y": down}, {"c": other}
    z_up, z_down = {"z": lax.rem(z + 1, NZ)}, {"z": lax.rem(z + NZ - 1, NZ)}
    z_others = [{"z": lax.rem(z + n, NZ)} for n in range(1, NZ)]
    x_others = [lax.rem(x + n, NX) for n in range(1, NX)]
    greet([to_up, to_down, to_other, z_up, z_down] + [{"x": n} for n in x_others])
    courier = Courier(ssem, rsem)
    send = courier.send
    loads[0].wait()

    first, second = pl.ds(0, HALF), pl.ds(HALF, HALF)

    def share(number, part, where):
        block = hbuf.at[number]
        if part is not None:
            block = block.at[part]
        return send(block, block, where)

    below, above, far = down * 2 + c, up * 2 + c, across * 2 + c
    below_first = share(own, first, to_up)
    above_second = share(own, second, to_down)
    below_second = share(own, second, to_up)
    above_first = share(own, first, to_down)
    beside = share(own, None, to_other)
    for load in loads[1:]:
        load.wait()

    def add(number, fresh=False):
        block = hbuf.at[number]
        at = pl.multiple_of(number * FEAT, FEAT)
        w = wbuf[pl.ds(at, FEAT), :]
        gain = gain_ref[:, pl.ds(at, FEAT)]

        @pl.loop(0, ROWS // 128)
        def _(t):
            rows = pl.ds(pl.multiple_of(t * 128, 128), 128)
            h = block[rows, :].astype(F32)
            squares = h[:, :128] * h[:, :128] + h[:, 128:] * h[:, 128:]
            product = dot((h * gain).astype(BF16), w)
            if fresh:
                sumsq[rows, :] = squares
                proj[rows, :] = product
            else:
                sumsq[rows, :] += squares
                proj[rows, :] += product

    add(own, True)
    beside.wait_recv()
    add(y * 2 + other)
    below_first.wait_recv()
    far_first = share(below, first, to_up)
    relays = [share(below, first, to_other)]
    above_second.wait_recv()
    far_second = share(above, second, to_down)
    relays.append(share(above, second, to_other))
    below_second.wait_recv()
    relays.append(share(below, second, to_other))
    above_first.wait_recv()
    relays.append(share(above, first, to_other))
    add(below)
    add(above)
    far_first.wait_recv()
    relays.append(share(far, first, to_other))
    far_second.wait_recv()
    relays.append(share(far, second, to_other))
    relays[0].wait_recv()
    relays[2].wait_recv()
    add(down * 2 + other)
    relays[1].wait_recv()
    relays[3].wait_recv()
    add(up * 2 + other)
    add(far)
    relays[4].wait_recv()
    relays[5].wait_recv()
    add(across * 2 + other)

    total = jnp.sum(sumsq[...], axis=1, keepdims=True)
    scale = lax.rsqrt(total * (1.0 / D) + NORM_EPS)
    k_ref[...] = (proj[:, 640:768] * scale).astype(BF16)
    vt_ref[...] = jnp.transpose(proj[:, 768:896] * scale).astype(BF16)
    q_ref[...] = (proj[:, 512:640] * (scale * (LOG2E * HD**-0.5))).astype(BF16)

    def pass_on(buf, source, slot, first, second):
        source[0].wait_recv()
        ahead = send(buf.at[slot - 1, first], buf.at[slot if slot < 3 else 6, first], z_up)
        source[1].wait_recv()
        back = send(buf.at[slot + 2, second], buf.at[slot + 3, second], z_down)
        return ahead, back

    key_all, value_all = pl.ds(0, ROWS), pl.ds(0, 128)
    keys = (send(k_ref, kbuf.at[0], z_up), send(k_ref, kbuf.at[3], z_down))
    values = (send(vt_ref, vbuf.at[0], z_up), send(vt_ref, vbuf.at[3], z_down))
    q_copies = [send(q_ref, qbuf.at[x], {"x": x_others[n]}) for n in (1, 0, 2)]

    @pl.loop(0, ROWS // 128)
    def _(t):
        rows = pl.ds(pl.multiple_of(t * 128, 128), 128)
        total = jnp.sum(sumsq[rows, :], axis=1, keepdims=True)
        scale = lax.rsqrt(total * (1.0 / D) + NORM_EPS)
        r_ref[rows, :] = (proj[rows, 0:128] * scale).astype(BF16)
        rk_ref[rows, :] = (proj[rows, 128:256] * scale).astype(BF16)
        rv_ref[rows, :] = (proj[rows, 256:384] * scale).astype(BF16)
        down_low = jnp.tanh(proj[rows, 384:512] * scale).astype(BF16)
        gate = dot(down_low, up_ref[...]) + base_ref[...]
        ld_ref[rows, :] = -DECAY_SCALE * jax.nn.sigmoid(gate) + shift_ref[rows, :]

    rate = rate_ref[...]
    so_far = None
    for n in range(ROWS // CHUNK):
        at = slice(n * CHUNK, (n + 1) * CHUNK)
        read_state, here, step = chunk_terms(
            r_ref[at, :].astype(F32),
            rk_ref[at, :].astype(F32),
            rv_ref[at, :],
            ld_ref[at, :],
            rate,
        )
        if so_far is None:
            reads[at, :] = read_state
            local[at, :] = here
            so_far = step
        else:
            seen = fine_dot(read_state, so_far)
            reads[at, :] = seen[:, :128]
            local[at, :] = here + seen[:, 128:]
            so_far = compose(step, so_far)
    gxsend[...] = packed(so_far)
    gxbuf[x] = packed(so_far)
    gx_copies = [send(gxsend, gxbuf.at[x], {"x": n}) for n in x_others]

    keys = pass_on(kbuf, keys, 1, key_all, key_all)
    values = pass_on(vbuf, values, 1, value_all, value_all)

    qbuf[x] = q_ref[...]
    for copy in q_copies:
        copy.wait_recv()
    for j in range(NX):
        qwide[j] = by_head(qbuf[j])
    tiles = [slice(t * 256, (t + 1) * 256) for t in range(3)]

    def attend_all(k_block, v_block, own):
        k_all, v_all = k_block[...], v_block[...]

        def scores_of(j):
            found = [dot_nt(k_all, qwide[j, cols, :]) for cols in tiles]
            if own:
                for t in range(3):
                    key_at = iota((ROWS, 256), 0)
                    query_at = lax.rem(iota((ROWS, 256), 1) + t * 256, ROWS)
                    keep = query_at - key_at >= (x - j) * ROWS
                    found[t] = jnp.where(keep, found[t], NEGATIVE)
            return found, [jnp.max(s, axis=0, keepdims=True) for s in found]

        ready = scores_of(0)
        for j in range(NX):
            following = scores_of(j + 1) if j + 1 < NX else None
            scores, highest = ready
            if not own:
                olds = [top[j, 0:1, cols] for cols in tiles]
                sums = [low[j, 0:1, cols] for cols in tiles]
                totals = [acc[j, :, cols] for cols in tiles]
            for t, cols in enumerate(tiles):
                new = highest[t] if own else jnp.maximum(olds[t], highest[t])
                weights = jnp.exp2(scores[t] - new)
                part = jnp.sum(weights, axis=0, keepdims=True)
                seen = dot(v_all, weights.astype(BF16))
                top[j, 0:1, cols] = new
                if own:
                    low[j, 0:1, cols] = part
                    acc[j, :, cols] = seen
                else:
                    rescale = jnp.exp2(olds[t] - new)
                    low[j, 0:1, cols] = sums[t] * rescale + part
                    acc[j, :, cols] = totals[t] * rescale + seen
            ready = following

    def attend(slot, needed):
        @pl.when(needed)
        def _():
            attend_all(kbuf.at[slot], vbuf.at[slot], False)

    attend_all(k_ref, vt_ref, True)
    attend(0, z >= 1)
    keys = pass_on(kbuf, keys, 2, key_all, key_all)
    attend(3, z >= NZ - 1)
    values = pass_on(vbuf, values, 2, value_all, value_all)

    for copy in gx_copies:
        copy.wait_recv()
    none = jnp.zeros((128, 128), F32)
    identity = jnp.where(iota((128, 256), 0) == iota((128, 256), 1), 1.0, 0.0)
    before_x = identity
    total = unpacked(gxbuf[0])
    for n in range(1, NX):
        before_x = jnp.where(x == n, total, before_x)
        total = compose(unpacked(gxbuf[n]), total)
    share = (packed(total) - packed_identity()).astype(BF16)
    gzsend[...] = share
    gzbuf[z] = share

    attend(1, z >= 2)
    keys = pass_on(kbuf, keys, 3, pl.ds(0, HALF), pl.ds(HALF, HALF))
    attend(4, z >= NZ - 2)
    values = pass_on(vbuf, values, 3, pl.ds(0, HD), pl.ds(HD, HD))
    attend(2, z >= 3)
    attend(5, z >= NZ - 3)
    for copy in (*keys, *values):
        copy.wait_recv()
    gz_copies = [send(gzsend, gzbuf.at[z], place) for place in z_others]
    attend(6, z >= 4)

    def partial_out(j):
        total = jnp.maximum(low[j, 0:1, :], TINY)
        return acc[j] * (1.0 / total), top[j, 0:1, :] + jnp.log2(total)

    o_copies = []
    for n in (1, 0, 2):
        j = x_others[n]
        out, level = partial_out(j)
        osend[n] = out.astype(BF16)
        stsend[n] = jnp.broadcast_to(level, (8, 2 * ROWS))
        o_copies.append(send(osend.at[n], orecv.at[n], {"x": j}))
        o_copies.append(send(stsend.at[n], strecv.at[n], {"x": j}))
    own_out, own_level = partial_out(x)

    for copy in gz_copies:
        copy.wait_recv()
    state = none
    for n in range(NZ - 1):
        step = unpacked(gzbuf[n].astype(F32) + packed_identity())
        after = fine_dot(step[:, :128], state) + step[:, 128:]
        state = jnp.where(n < z, after, state)
    state = fine_dot(before_x[:, :128], state) + before_x[:, 128:]
    recurrent = local[...] + fine_dot(reads[...], state)
    first = iota((ROWS, 128), 1) < HD

    def head_mean(values):
        one = jnp.sum(jnp.where(first, values, 0.0), axis=1, keepdims=True)
        two = jnp.sum(jnp.where(first, 0.0, values), axis=1, keepdims=True)
        return jnp.where(first, one, two) * (1.0 / HD)

    centered = recurrent - head_mean(recurrent)
    normal = centered * lax.rsqrt(head_mean(centered * centered) + GROUP_EPS)
    mix_ref[:, 0:128] = normal.astype(BF16)

    for copy in o_copies:
        copy.wait_recv()
    levels = [own_level] + [strecv[n, 0:1, :] for n in range(3)]
    highest = functools.reduce(jnp.maximum, levels)
    shares = [jnp.exp2(level - highest) for level in levels]
    share_sum = sum(shares)
    map_out = own_out * (shares[0] / share_sum)
    for n in range(3):
        map_out = map_out + orecv[n].astype(F32) * (shares[n + 1] / share_sum)
    sums = (highest + jnp.log2(share_sum)) * LN2
    sums_ref[0:1, :] = sums[:, :ROWS]
    sums_ref[1:2, :] = sums[:, ROWS:]
    head_out = map_out[:, :ROWS] - lam_ref[0] * map_out[:, ROWS:]
    head_out = head_out * lax.rsqrt(
        jnp.mean(head_out * head_out, axis=0, keepdims=True) + HEAD_EPS
    )
    mix_ref[:, 128:256] = jnp.transpose(head_out).astype(BF16)

    part_rows = ROWS // (NY * NC)
    order = [across, up, down, y]

    def rows_for(core):
        return jnp.concatenate(
            [
                mix_ref[pl.ds(pl.multiple_of((n * 2 + core) * part_rows, part_rows), part_rows), :]
                for n in order
            ],
            0,
        )

    theirs = rows_for(other)
    ours = rows_for(c)
    for t in range(8):
        cols = slice(t * 256, (t + 1) * 256)
        psend[:, cols] = dot(theirs, out_w[:, cols]).astype(BF16)
    pairs = [
        send(psend.at[pl.ds(n * part_rows, part_rows)], precv.at[pl.ds(n * part_rows, part_rows)], to_other)
        for n in range(4)
    ]
    for t in range(8):
        cols = slice(t * 256, (t + 1) * 256)
        pair[:, cols] = dot(ours, out_w[:, cols])
    one, two = slice(0, D // 2), slice(D // 2, D)

    def summed(n, half):
        at = slice(n * part_rows, (n + 1) * part_rows)
        return pair[at, half] + precv[at, half].astype(F32)

    pairs[0].wait_recv()
    hsend[0] = summed(0, one).astype(BF16)
    relay_up = send(hsend.at[0], hrecv.at[0], to_up)
    hsend[1] = summed(0, two).astype(BF16)
    relay_down = send(hsend.at[1], hrecv.at[1], to_down)
    pairs[1].wait_recv()
    hsend[2] = summed(1, two).astype(BF16)
    plain_up = send(hsend.at[2], hrecv.at[2], to_up)
    pairs[2].wait_recv()
    hsend[3] = summed(2, one).astype(BF16)
    plain_down = send(hsend.at[3], hrecv.at[3], to_down)
    relay_up.wait_recv()
    hsend[4] = (summed(1, one) + hrecv[0].astype(F32)).astype(BF16)
    merged_up = send(hsend.at[4], hrecv.at[4], to_up)
    relay_down.wait_recv()
    hsend[5] = (summed(2, two) + hrecv[1].astype(F32)).astype(BF16)
    merged_down = send(hsend.at[5], hrecv.at[5], to_down)
    pairs[3].wait_recv()
    plain_up.wait_recv()
    plain_down.wait_recv()
    left_half = summed(3, one) + hrecv[3].astype(F32)
    right_half = summed(3, two) + hrecv[2].astype(F32)
    merged_up.wait_recv()
    merged_down.wait_recv()
    left_half = left_half + hrecv[4].astype(F32)
    right_half = right_half + hrecv[5].astype(F32)
    total = jnp.sum(left_half * left_half, axis=1, keepdims=True) + jnp.sum(
        right_half * right_half, axis=1, keepdims=True
    )
    scale = lax.rsqrt(total * (1.0 / D) + NORM_EPS)
    out_ref[:, one] = (left_half * scale * out_gain_ref[:, one]).astype(BF16)
    out_ref[:, two] = (right_half * scale * out_gain_ref[:, two]).astype(BF16)
    for copy in courier.copies:
        copy.wait_send()


def run_layer(lam, hid, gain, up, base, shift, rate, wr, wa, out_gain, weights):
    whole = pl.BlockSpec(memory_space=VMEM)
    far = pl.BlockSpec(memory_space=pl.ANY)
    share = ROWS // (NY * NC)
    count = 13 + 16 + 3 + 3 + 7 + 6 + 10
    rows = VMEM((ROWS, 128), BF16)
    return pl.pallas_call(
        layer,
        out_shape=(
            jax.ShapeDtypeStruct((share, D), BF16),
            jax.ShapeDtypeStruct((2, ROWS), F32),
        ),
        in_specs=[pl.BlockSpec(memory_space=pltpu.SMEM)] + [far] * 16,
        out_specs=(whole, whole),
        scratch_shapes=[
            VMEM((NY * NC, ROWS, FEAT), BF16),
            VMEM((D, 896), BF16),
            VMEM((ROWS, 896), F32),
            VMEM((ROWS, 128), F32),
            VMEM((1, D), F32),
            VMEM((128, 128), BF16),
            VMEM((1, 128), F32),
            VMEM((ROWS, 128), F32),
            VMEM((1, 128), F32),
            VMEM((256, D), BF16),
            VMEM((1, D), F32),
            rows,
            rows,
            VMEM((128, ROWS), BF16),
            rows,
            rows,
            rows,
            VMEM((ROWS, 128), F32),
            VMEM((7, ROWS, 128), BF16),
            VMEM((7, 128, ROWS), BF16),
            VMEM((NX, ROWS, 128), BF16),
            VMEM((NX, 2 * ROWS, 128), BF16),
            VMEM((NX, 128, 2 * ROWS), F32),
            VMEM((NX, 8, 2 * ROWS), F32),
            VMEM((NX, 8, 2 * ROWS), F32),
            VMEM((3, 128, 2 * ROWS), BF16),
            VMEM((3, 128, 2 * ROWS), BF16),
            VMEM((3, 8, 2 * ROWS), F32),
            VMEM((3, 8, 2 * ROWS), F32),
            VMEM((HD, 256), F32),
            VMEM((NX, HD, 256), F32),
            VMEM((HD, 256), BF16),
            VMEM((NZ, HD, 256), BF16),
            VMEM((ROWS, 128), F32),
            VMEM((ROWS, 128), F32),
            VMEM((ROWS, 256), BF16),
            VMEM((4 * share, D), BF16),
            VMEM((4 * share, D), BF16),
            VMEM((4 * share, D), F32),
            VMEM((6, share, D // 2), BF16),
            VMEM((6, share, D // 2), BF16),
            pltpu.SemaphoreType.DMA((16,)),
            pltpu.SemaphoreType.DMA((count,)),
            pltpu.SemaphoreType.DMA((count,)),
        ],
        compiler_params=pltpu.CompilerParams(
            collective_id=0, has_side_effects=True, vmem_limit_bytes=63 * 2**20
        ),
        name="layer",
    )(lam, hid, gain, up, base, shift, rate, wr, wa, out_gain, *weights)


def per_device(
    hidden_in,
    in_gain,
    receptance_weight,
    key_weight,
    value_weight,
    decay_down,
    decay_up,
    decay_base,
    decay_shift,
    learn_rate,
    query_pair,
    key_pair,
    value_pair,
    mix_lambda,
    out_recurrent,
    out_attention,
    out_gain,
):
    layer_out, sums = run_layer(
        mix_lambda,
        hidden_in,
        in_gain.reshape(1, D),
        decay_up,
        decay_base.reshape(1, 128),
        decay_shift,
        learn_rate.reshape(1, 128),
        out_recurrent,
        out_attention,
        out_gain.reshape(1, D),
        (
            receptance_weight,
            key_weight,
            value_weight,
            decay_down,
            query_pair.reshape(D, 128),
            key_pair.reshape(D, 128),
            value_pair.reshape(D, 128),
        ),
    )
    return layer_out, sums.reshape(1, 2, ROWS)


def solution(mesh):
    split_mesh = Mesh(mesh.devices.reshape(NZ, NX, NY, NC), ("z", "x", "y", "c"))
    sp, tp = ("z", "x"), ("y", "c")
    placed = (
        P(sp, tp),
        P(),
        P(None, tp),
        P(None, tp),
        P(None, tp),
        P(),
        P(None, tp),
        P(tp),
        P(sp, tp),
        P(tp),
        P(None, tp, None),
        P(None, tp, None),
        P(None, tp, None),
        P(tp),
        P(tp, None),
        P(tp, None),
        P(),
    )
    return jax.shard_map(
        per_device,
        mesh=split_mesh,
        in_specs=placed,
        out_specs=(P((*sp, *tp), None), P(tp, None, sp)),
        check_vma=False,
    )
```

```python
import functools
import math

import jax
import jax.numpy as jnp
from jax import lax
from jax.experimental import pallas as pl
from jax.experimental.pallas import tpu as pltpu
from jax.sharding import Mesh
from jax.sharding import PartitionSpec as P

F32 = jnp.float32
BF16 = jnp.bfloat16
HD = 64
NZ, NX, NY, NC = 8, 4, 4, 2
ROWS = 384
HALF = ROWS // 2
D = 2048
FEAT = 256
CHUNK = 128
SUB = 32
DECAY_SCALE = math.exp(-0.5)
NORM_EPS = 1e-06
GROUP_EPS = 0.00064
HEAD_EPS = 1e-05
KEY_EPS = 1e-06
NEGATIVE = -1e30
TINY = 1e-37
LOG2E = 1.4426950408889634
LN2 = 0.6931471805599453
MESH = pl.DeviceIdType.MESH
VMEM = pltpu.VMEM
HIGHEST = lax.Precision.HIGHEST


def dot(a, b):
    return jnp.dot(a, b, preferred_element_type=F32)


def dot_nt(a, b):
    return lax.dot_general(a, b, (((1,), (1,)), ((), ())), preferred_element_type=F32)


def split(x):
    high = x.astype(BF16)
    return high, (x - high.astype(F32)).astype(BF16)


def fine_dot(a, b):
    a_high, a_low = split(a)
    b_high, b_low = split(b)
    both = dot(jnp.concatenate([a_high, a_low], 1), jnp.concatenate([b_high, b_high], 0))
    return both + dot(a_high, b_low)


def fine_dot_nt(a, b):
    a_high, a_low = split(a)
    b_high, b_low = split(b)
    both = dot_nt(jnp.concatenate([a_high, a_low], 1), jnp.concatenate([b_high, b_high], 1))
    return both + dot_nt(a_high, b_low)


def coarse_dot(a, b):
    return dot(a.astype(BF16), b.astype(BF16))


def remote(src, dst, send_sem, recv_sem, where):
    return pltpu.make_async_remote_copy(
        src_ref=src,
        dst_ref=dst,
        send_sem=send_sem,
        recv_sem=recv_sem,
        device_id=where,
        device_id_type=MESH,
    )


def greet(places):
    barrier = pltpu.get_barrier_semaphore()
    for place in places:
        pl.semaphore_signal(barrier, inc=1, device_id=place, device_id_type=MESH)
    pl.semaphore_wait(barrier, len(places))


def iota(shape, dim):
    return lax.broadcasted_iota(jnp.int32, shape, dim)


def by_head(x):
    first = lax.rem(iota(x.shape, 1), 128) < HD
    zero = jnp.zeros_like(x)
    return jnp.concatenate([jnp.where(first, x, zero), jnp.where(first, zero, x)], 0)


def same_head(shape):
    return (iota(shape, 0) < HD) == (lax.rem(iota(shape, 1), 128) < HD)


SIZES = ((1, 8), (8, 32), (32, 128))


def blocks_mask(small, large):
    row, col = iota((CHUNK, CHUNK), 0), iota((CHUNK, CHUNK), 1)
    return (lax.div(row, large) == lax.div(col, large)) & (lax.div(row, small) > lax.div(col, small))


def inverses(lowers):
    row, col = iota((CHUNK, CHUNK), 0), iota((CHUNK, CHUNK), 1)
    identity = jnp.where(row == col, 1.0, 0.0)
    found = None
    for small, large in SIZES:
        keep = blocks_mask(small, large)
        parts = [jnp.where(keep, lower, 0.0) for lower in lowers]
        if found is None:
            steps = parts
            found = [identity + part for part in parts]
        else:
            steps = [coarse_dot(f, part) for f, part in zip(found, parts)]
            found = [f + coarse_dot(s, f) for f, s in zip(found, steps)]
        reach = 2
        while reach * small < large:
            steps = [coarse_dot(s, s) for s in steps]
            found = [f + coarse_dot(s, f) for f, s in zip(found, steps)]
            reach *= 2
    return found


def all_terms(receptance, keys, values, decays, rate):
    count = ROWS // CHUNK
    cuts = [slice(n * CHUNK, (n + 1) * CHUNK) for n in range(count)]
    row, col = iota((CHUNK, CHUNK), 0), iota((CHUNK, CHUNK), 1)
    ones = (row >= col).astype(BF16)
    first = col < HD
    w = [decays[at, :] for at in cuts]
    r = [receptance[at, :].astype(F32) for at in cuts]
    k = [keys[at, :].astype(F32) for at in cuts]
    v = [values[at, :] for at in cuts]
    running = []
    for part in w:
        high = part.astype(BF16)
        rest = part - high.astype(F32)
        middle = rest.astype(BF16)
        lowest = (rest - middle.astype(F32)).astype(BF16)
        running.append(
            dot(jnp.concatenate([ones, ones], 1), jnp.concatenate([high, middle], 0))
            + dot(ones, lowest)
        )
    before = [a - b for a, b in zip(running, w)]
    ending = [a[CHUNK - 1 :, :] for a in running]
    unit = []
    for part in k:
        square = part * part
        one = jnp.sum(jnp.where(first, square, 0.0), axis=1, keepdims=True)
        two = jnp.sum(jnp.where(first, 0.0, square), axis=1, keepdims=True)
        unit.append(part * lax.rsqrt(jnp.where(first, one, two) + KEY_EPS))
    erasing = [u * rate for u in unit]
    pieces = [[] for _ in cuts]
    for i in range(CHUNK // SUB):
        at = slice(i * SUB, (i + 1) * SUB)
        for n in range(count):
            start = running[n][i * SUB - 1 : i * SUB, :] if i else jnp.zeros_like(ending[n])
            left = jnp.concatenate(
                [
                    -unit[n][at] * jnp.exp(before[n][at] - start),
                    r[n][at] * jnp.exp(running[n][at] - start),
                ],
                0,
            )
            growth = jnp.exp(jnp.where(row < (i + 1) * SUB, start - running[n], -100.0))
            right = jnp.concatenate([erasing[n] * growth, k[n] * growth], 0)
            pieces[n].append(fine_dot_nt(by_head(left), right))

    def matrix(n, head, read, which, keep):
        at = head * 2 * SUB + read * SUB
        whole = jnp.concatenate(
            [p[at : at + SUB, which * CHUNK : (which + 1) * CHUNK] for p in pieces[n]], 0
        )
        return jnp.where(keep, whole, 0.0)

    strict, causal = row > col, row >= col
    found = inverses([matrix(n, h, 0, 0, strict) for n in range(count) for h in range(2)])
    found = [jnp.concatenate(found[2 * n : 2 * n + 2], 1) for n in range(count)]

    def pair(n, read, which, keep):
        return jnp.concatenate(
            [matrix(n, h, read, which, keep).astype(BF16) for h in range(2)], 1
        )

    by_value = [by_head(part) for part in v]
    carried = [dot(pair(n, 0, 1, strict), by_value[n]) for n in range(count)]
    right_side = [
        by_head(jnp.concatenate([-unit[n] * jnp.exp(before[n]), carried[n]], 1))
        for n in range(count)
    ]
    solved = [fine_dot(found[n], right_side[n]) for n in range(count)]
    seen = [
        dot(pair(n, 1, 0, causal), by_head(solved[n].astype(BF16))) for n in range(count)
    ]
    local = [seen[n][:, 128:] + dot(pair(n, 1, 1, causal), by_value[n]) for n in range(count)]
    read_state = [r[n] * jnp.exp(running[n]) + seen[n][:, :128] for n in range(count)]
    none = jnp.zeros((CHUNK, 128), F32)
    wide_row, wide_col = iota((128, 256), 0), iota((128, 256), 1)
    steps = []
    for n in range(count):
        to_end = jnp.exp(ending[n] - running[n])
        left = jnp.concatenate(
            [jnp.transpose(erasing[n] * to_end), jnp.transpose(k[n] * to_end)], 1
        )
        right = jnp.concatenate(
            [solved[n], jnp.concatenate([none, v[n].astype(F32)], 1)], 0
        )
        step = jnp.where(same_head((128, 256)), fine_dot(left, right), 0.0)
        decayed = jnp.concatenate(
            [jnp.broadcast_to(jnp.exp(ending[n]), (128, 128)), none], 1
        )
        steps.append(step + jnp.where(wide_row == wide_col, decayed, 0.0))
    return read_state, local, steps


def device_terms(receptance, keys, values, decays, rate):
    read_state, local, steps = all_terms(receptance, keys, values, decays, rate)
    reads, reach = [read_state[0]], [local[0]]
    so_far = steps[0]
    for n in range(1, len(steps)):
        seen = fine_dot(read_state[n], so_far)
        reads.append(seen[:, :128])
        reach.append(local[n] + seen[:, 128:])
        so_far = compose(steps[n], so_far)
    return reads, reach, so_far


def compose(later, earlier):
    out = fine_dot(later[:, :128], earlier)
    none = jnp.zeros((128, 128), F32)
    return out + jnp.concatenate([none, later[:, 128:]], 1)


def packed(step):
    return step[:HD] + step[HD:]


def unpacked(step):
    both = jnp.concatenate([step, step], 0)
    return jnp.where(same_head((128, 256)), both, 0.0)


def packed_identity():
    row, col = iota((HD, 256), 0), iota((HD, 256), 1)
    return jnp.where((col < 128) & (lax.rem(col, HD) == row), 1.0, 0.0)


class Courier:
    def __init__(self, ssem, rsem):
        self.ssem, self.rsem, self.copies = ssem, rsem, []

    def send(self, src, dst, where):
        n = len(self.copies)
        copy = remote(src, dst, self.ssem.at[n], self.rsem.at[n], where)
        copy.start()
        self.copies.append(copy)
        return copy


def load_all(places, sems, first):
    loads = []
    for n, (src, dst) in enumerate(places):
        load = pltpu.make_async_copy(src, dst, sems.at[first + n])
        load.start()
        loads.append(load)
    return loads


def layer(
    lam_ref,
    hid_hbm,
    gain_hbm,
    up_hbm,
    base_hbm,
    shift_hbm,
    rate_hbm,
    wr_hbm,
    wa_hbm,
    out_gain_hbm,
    *rest,
):
    weights = rest[:7]
    out_ref, sums_ref = rest[7:9]
    (
        hbuf,
        wbuf,
        proj,
        sumsq,
        gain_ref,
        up_ref,
        base_ref,
        shift_ref,
        rate_ref,
        out_w,
        out_gain_ref,
        q_ref,
        k_ref,
        vt_ref,
        r_ref,
        rk_ref,
        rv_ref,
        ld_ref,
        kbuf,
        vbuf,
        qbuf,
        qwide,
        acc,
        top,
        low,
        osend,
        orecv,
        stsend,
        strecv,
        gxsend,
        gxbuf,
        gzsend,
        gzbuf,
        reads,
        local,
        mix_ref,
        psend,
        precv,
        pair,
        hsend,
        hrecv,
        wsem,
        ssem,
        rsem,
    ) = rest[9:]
    z = lax.axis_index("z")
    x = lax.axis_index("x")
    y = lax.axis_index("y")
    c = lax.axis_index("c")
    other = 1 - c
    up, down, across = lax.rem(y + 1, NY), lax.rem(y + 3, NY), lax.rem(y + 2, NY)
    own = y * 2 + c
    loads = load_all([(hid_hbm, hbuf.at[own])], wsem, 0)
    places = [(w, wbuf.at[:, pl.ds(n * 128, 128)]) for n, w in enumerate(weights)]
    places += [
        (gain_hbm, gain_ref),
        (up_hbm, up_ref),
        (base_hbm, base_ref),
        (shift_hbm, shift_ref),
        (rate_hbm, rate_ref),
        (wr_hbm, out_w.at[pl.ds(0, 128)]),
        (wa_hbm, out_w.at[pl.ds(128, 128)]),
        (out_gain_hbm, out_gain_ref),
    ]
    loads += load_all(places, wsem, 1)
    to_up, to_down, to_other = {"y": up}, {"y": down}, {"c": other}
    z_up, z_down = {"z": lax.rem(z + 1, NZ)}, {"z": lax.rem(z + NZ - 1, NZ)}
    z_others = [{"z": lax.rem(z + n, NZ)} for n in range(1, NZ)]
    x_others = [lax.rem(x + n, NX) for n in range(1, NX)]
    greet([to_up, to_down, to_other, z_up, z_down] + [{"x": n} for n in x_others])
    courier = Courier(ssem, rsem)
    send = courier.send
    loads[0].wait()

    first, second = pl.ds(0, HALF), pl.ds(HALF, HALF)

    def share(number, part, where):
        block = hbuf.at[number]
        if part is not None:
            block = block.at[part]
        return send(block, block, where)

    below, above, far = down * 2 + c, up * 2 + c, across * 2 + c
    below_first = share(own, first, to_up)
    above_second = share(own, second, to_down)
    below_second = share(own, second, to_up)
    above_first = share(own, first, to_down)
    beside = share(own, None, to_other)
    for load in loads[1:]:
        load.wait()

    def add(number, fresh=False):
        block = hbuf.at[number]
        at = pl.multiple_of(number * FEAT, FEAT)
        w = wbuf[pl.ds(at, FEAT), :]
        gain = gain_ref[:, pl.ds(at, FEAT)]

        @pl.loop(0, ROWS // 128)
        def _(t):
            rows = pl.ds(pl.multiple_of(t * 128, 128), 128)
            h = block[rows, :].astype(F32)
            squares = h[:, :128] * h[:, :128] + h[:, 128:] * h[:, 128:]
            product = dot((h * gain).astype(BF16), w)
            if fresh:
                sumsq[rows, :] = squares
                proj[rows, :] = product
            else:
                sumsq[rows, :] += squares
                proj[rows, :] += product

    add(own, True)
    beside.wait_recv()
    add(y * 2 + other)
    below_first.wait_recv()
    far_first = share(below, first, to_up)
    relays = [share(below, first, to_other)]
    above_second.wait_recv()
    far_second = share(above, second, to_down)
    relays.append(share(above, second, to_other))
    below_second.wait_recv()
    relays.append(share(below, second, to_other))
    above_first.wait_recv()
    relays.append(share(above, first, to_other))
    add(below)
    add(above)
    far_first.wait_recv()
    relays.append(share(far, first, to_other))
    far_second.wait_recv()
    relays.append(share(far, second, to_other))
    relays[0].wait_recv()
    relays[2].wait_recv()
    add(down * 2 + other)
    relays[1].wait_recv()
    relays[3].wait_recv()
    add(up * 2 + other)
    add(far)
    relays[4].wait_recv()
    relays[5].wait_recv()
    add(across * 2 + other)

    total = jnp.sum(sumsq[...], axis=1, keepdims=True)
    scale = lax.rsqrt(total * (1.0 / D) + NORM_EPS)
    k_ref[...] = (proj[:, 640:768] * scale).astype(BF16)
    vt_ref[...] = jnp.transpose(proj[:, 768:896] * scale).astype(BF16)
    q_ref[...] = (proj[:, 512:640] * (scale * (LOG2E * HD**-0.5))).astype(BF16)

    def pass_on(buf, source, slot, first, second):
        source[0].wait_recv()
        ahead = send(buf.at[slot - 1, first], buf.at[slot if slot < 3 else 6, first], z_up)
        source[1].wait_recv()
        back = send(buf.at[slot + 2, second], buf.at[slot + 3, second], z_down)
        return ahead, back

    key_all, value_all = pl.ds(0, ROWS), pl.ds(0, 128)
    keys = (send(k_ref, kbuf.at[0], z_up), send(k_ref, kbuf.at[3], z_down))
    values = (send(vt_ref, vbuf.at[0], z_up), send(vt_ref, vbuf.at[3], z_down))
    q_copies = [send(q_ref, qbuf.at[x], {"x": x_others[n]}) for n in (1, 0, 2)]

    @pl.loop(0, ROWS // 128)
    def _(t):
        rows = pl.ds(pl.multiple_of(t * 128, 128), 128)
        total = jnp.sum(sumsq[rows, :], axis=1, keepdims=True)
        scale = lax.rsqrt(total * (1.0 / D) + NORM_EPS)
        r_ref[rows, :] = (proj[rows, 0:128] * scale).astype(BF16)
        rk_ref[rows, :] = (proj[rows, 128:256] * scale).astype(BF16)
        rv_ref[rows, :] = (proj[rows, 256:384] * scale).astype(BF16)
        down_low = jnp.tanh(proj[rows, 384:512] * scale).astype(BF16)
        gate = dot(down_low, up_ref[...]) + base_ref[...]
        ld_ref[rows, :] = -DECAY_SCALE * jax.nn.sigmoid(gate) + shift_ref[rows, :]

    found_reads, found_local, so_far = device_terms(r_ref, rk_ref, rv_ref, ld_ref, rate_ref[...])
    for n in range(ROWS // CHUNK):
        reads[n * CHUNK : (n + 1) * CHUNK, :] = found_reads[n]
        local[n * CHUNK : (n + 1) * CHUNK, :] = found_local[n]
    gxsend[...] = packed(so_far)
    gxbuf[x] = packed(so_far)
    gx_copies = [send(gxsend, gxbuf.at[x], {"x": n}) for n in x_others]

    keys = pass_on(kbuf, keys, 1, key_all, key_all)
    values = pass_on(vbuf, values, 1, value_all, value_all)

    qbuf[x] = q_ref[...]
    for copy in q_copies:
        copy.wait_recv()
    for j in range(NX):
        qwide[j] = by_head(qbuf[j])
    tiles = [slice(t * 256, (t + 1) * 256) for t in range(3)]

    def attend_all(k_block, v_block, own):
        k_all, v_all = k_block[...], v_block[...]

        def scores_of(j):
            found = [dot_nt(k_all, qwide[j, cols, :]) for cols in tiles]
            if own:
                for t in range(3):
                    key_at = iota((ROWS, 256), 0)
                    query_at = lax.rem(iota((ROWS, 256), 1) + t * 256, ROWS)
                    keep = query_at - key_at >= (x - j) * ROWS
                    found[t] = jnp.where(keep, found[t], NEGATIVE)
            return found, [jnp.max(s, axis=0, keepdims=True) for s in found]

        ready = scores_of(0)
        for j in range(NX):
            following = scores_of(j + 1) if j + 1 < NX else None
            scores, highest = ready
            if not own:
                olds = [top[j, 0:1, cols] for cols in tiles]
                sums = [low[j, 0:1, cols] for cols in tiles]
                totals = [acc[j, :, cols] for cols in tiles]
            for t, cols in enumerate(tiles):
                new = highest[t] if own else jnp.maximum(olds[t], highest[t])
                weights = jnp.exp2(scores[t] - new)
                part = jnp.sum(weights, axis=0, keepdims=True)
                seen = dot(v_all, weights.astype(BF16))
                top[j, 0:1, cols] = new
                if own:
                    low[j, 0:1, cols] = part
                    acc[j, :, cols] = seen
                else:
                    rescale = jnp.exp2(olds[t] - new)
                    low[j, 0:1, cols] = sums[t] * rescale + part
                    acc[j, :, cols] = totals[t] * rescale + seen
            ready = following

    def attend(slot, needed):
        @pl.when(needed)
        def _():
            attend_all(kbuf.at[slot], vbuf.at[slot], False)

    attend_all(k_ref, vt_ref, True)
    attend(0, z >= 1)
    keys = pass_on(kbuf, keys, 2, key_all, key_all)
    attend(3, z >= NZ - 1)
    values = pass_on(vbuf, values, 2, value_all, value_all)

    for copy in gx_copies:
        copy.wait_recv()
    none = jnp.zeros((128, 128), F32)
    identity = jnp.where(iota((128, 256), 0) == iota((128, 256), 1), 1.0, 0.0)
    before_x = identity
    total = unpacked(gxbuf[0])
    for n in range(1, NX):
        before_x = jnp.where(x == n, total, before_x)
        total = compose(unpacked(gxbuf[n]), total)
    share = (packed(total) - packed_identity()).astype(BF16)
    gzsend[...] = share
    gzbuf[z] = share

    attend(1, z >= 2)
    keys = pass_on(kbuf, keys, 3, pl.ds(0, HALF), pl.ds(HALF, HALF))
    attend(4, z >= NZ - 2)
    values = pass_on(vbuf, values, 3, pl.ds(0, HD), pl.ds(HD, HD))
    attend(2, z >= 3)
    attend(5, z >= NZ - 3)
    for copy in (*keys, *values):
        copy.wait_recv()
    gz_copies = [send(gzsend, gzbuf.at[z], place) for place in z_others]
    attend(6, z >= 4)

    def partial_out(j):
        total = jnp.maximum(low[j, 0:1, :], TINY)
        return acc[j] * (1.0 / total), top[j, 0:1, :] + jnp.log2(total)

    o_copies = []
    for n in (1, 0, 2):
        j = x_others[n]
        out, level = partial_out(j)
        osend[n] = out.astype(BF16)
        stsend[n] = jnp.broadcast_to(level, (8, 2 * ROWS))
        o_copies.append(send(osend.at[n], orecv.at[n], {"x": j}))
        o_copies.append(send(stsend.at[n], strecv.at[n], {"x": j}))
    own_out, own_level = partial_out(x)

    for copy in gz_copies:
        copy.wait_recv()
    state = none
    for n in range(NZ - 1):
        step = unpacked(gzbuf[n].astype(F32) + packed_identity())
        after = fine_dot(step[:, :128], state) + step[:, 128:]
        state = jnp.where(n < z, after, state)
    state = fine_dot(before_x[:, :128], state) + before_x[:, 128:]
    recurrent = local[...] + fine_dot(reads[...], state)
    first = iota((ROWS, 128), 1) < HD

    def head_mean(values):
        one = jnp.sum(jnp.where(first, values, 0.0), axis=1, keepdims=True)
        two = jnp.sum(jnp.where(first, 0.0, values), axis=1, keepdims=True)
        return jnp.where(first, one, two) * (1.0 / HD)

    centered = recurrent - head_mean(recurrent)
    normal = centered * lax.rsqrt(head_mean(centered * centered) + GROUP_EPS)
    mix_ref[:, 0:128] = normal.astype(BF16)

    for copy in o_copies:
        copy.wait_recv()
    levels = [own_level] + [strecv[n, 0:1, :] for n in range(3)]
    highest = functools.reduce(jnp.maximum, levels)
    shares = [jnp.exp2(level - highest) for level in levels]
    share_sum = sum(shares)
    map_out = own_out * (shares[0] / share_sum)
    for n in range(3):
        map_out = map_out + orecv[n].astype(F32) * (shares[n + 1] / share_sum)
    sums = (highest + jnp.log2(share_sum)) * LN2
    sums_ref[0, 0:1, :] = sums[:, :ROWS]
    sums_ref[0, 1:2, :] = sums[:, ROWS:]
    head_out = map_out[:, :ROWS] - lam_ref[0] * map_out[:, ROWS:]
    head_out = head_out * lax.rsqrt(
        jnp.mean(head_out * head_out, axis=0, keepdims=True) + HEAD_EPS
    )
    mix_ref[:, 128:256] = jnp.transpose(head_out).astype(BF16)

    part_rows = ROWS // (NY * NC)
    order = [across, up, down, y]

    def rows_for(core):
        return jnp.concatenate(
            [
                mix_ref[pl.ds(pl.multiple_of((n * 2 + core) * part_rows, part_rows), part_rows), :]
                for n in order
            ],
            0,
        )

    theirs = rows_for(other)
    ours = rows_for(c)
    for t in range(8):
        cols = slice(t * 256, (t + 1) * 256)
        psend[:, cols] = dot(theirs, out_w[:, cols]).astype(BF16)
    pairs = [
        send(psend.at[pl.ds(n * part_rows, part_rows)], precv.at[pl.ds(n * part_rows, part_rows)], to_other)
        for n in range(4)
    ]
    for t in range(8):
        cols = slice(t * 256, (t + 1) * 256)
        pair[:, cols] = dot(ours, out_w[:, cols])
    one, two = slice(0, D // 2), slice(D // 2, D)

    def summed(n, half):
        at = slice(n * part_rows, (n + 1) * part_rows)
        return pair[at, half] + precv[at, half].astype(F32)

    pairs[0].wait_recv()
    hsend[0] = summed(0, one).astype(BF16)
    relay_up = send(hsend.at[0], hrecv.at[0], to_up)
    hsend[1] = summed(0, two).astype(BF16)
    relay_down = send(hsend.at[1], hrecv.at[1], to_down)
    pairs[1].wait_recv()
    hsend[2] = summed(1, two).astype(BF16)
    plain_up = send(hsend.at[2], hrecv.at[2], to_up)
    pairs[2].wait_recv()
    hsend[3] = summed(2, one).astype(BF16)
    plain_down = send(hsend.at[3], hrecv.at[3], to_down)
    relay_up.wait_recv()
    hsend[4] = (summed(1, one) + hrecv[0].astype(F32)).astype(BF16)
    merged_up = send(hsend.at[4], hrecv.at[4], to_up)
    relay_down.wait_recv()
    hsend[5] = (summed(2, two) + hrecv[1].astype(F32)).astype(BF16)
    merged_down = send(hsend.at[5], hrecv.at[5], to_down)
    pairs[3].wait_recv()
    plain_up.wait_recv()
    plain_down.wait_recv()
    left_half = summed(3, one) + hrecv[3].astype(F32)
    right_half = summed(3, two) + hrecv[2].astype(F32)
    merged_up.wait_recv()
    merged_down.wait_recv()
    left_half = left_half + hrecv[4].astype(F32)
    right_half = right_half + hrecv[5].astype(F32)
    total = jnp.sum(left_half * left_half, axis=1, keepdims=True) + jnp.sum(
        right_half * right_half, axis=1, keepdims=True
    )
    scale = lax.rsqrt(total * (1.0 / D) + NORM_EPS)
    out_ref[:, one] = (left_half * scale * out_gain_ref[:, one]).astype(BF16)
    out_ref[:, two] = (right_half * scale * out_gain_ref[:, two]).astype(BF16)
    for copy in courier.copies:
        copy.wait_send()


def run_layer(lam, hid, gain, up, base, shift, rate, wr, wa, out_gain, weights):
    whole = pl.BlockSpec(memory_space=VMEM)
    far = pl.BlockSpec(memory_space=pl.ANY)
    share = ROWS // (NY * NC)
    count = 13 + 16 + 3 + 3 + 7 + 6 + 10
    rows = VMEM((ROWS, 128), BF16)
    return pl.pallas_call(
        layer,
        out_shape=(
            jax.ShapeDtypeStruct((share, D), BF16),
            jax.ShapeDtypeStruct((1, 2, ROWS), F32),
        ),
        in_specs=[pl.BlockSpec(memory_space=pltpu.SMEM)] + [far] * 16,
        out_specs=(whole, whole),
        scratch_shapes=[
            VMEM((NY * NC, ROWS, FEAT), BF16),
            VMEM((D, 896), BF16),
            VMEM((ROWS, 896), F32),
            VMEM((ROWS, 128), F32),
            VMEM((1, D), F32),
            VMEM((128, 128), BF16),
            VMEM((1, 128), F32),
            VMEM((ROWS, 128), F32),
            VMEM((1, 128), F32),
            VMEM((256, D), BF16),
            VMEM((1, D), F32),
            rows,
            rows,
            VMEM((128, ROWS), BF16),
            rows,
            rows,
            rows,
            VMEM((ROWS, 128), F32),
            VMEM((7, ROWS, 128), BF16),
            VMEM((7, 128, ROWS), BF16),
            VMEM((NX, ROWS, 128), BF16),
            VMEM((NX, 2 * ROWS, 128), BF16),
            VMEM((NX, 128, 2 * ROWS), F32),
            VMEM((NX, 8, 2 * ROWS), F32),
            VMEM((NX, 8, 2 * ROWS), F32),
            VMEM((3, 128, 2 * ROWS), BF16),
            VMEM((3, 128, 2 * ROWS), BF16),
            VMEM((3, 8, 2 * ROWS), F32),
            VMEM((3, 8, 2 * ROWS), F32),
            VMEM((HD, 256), F32),
            VMEM((NX, HD, 256), F32),
            VMEM((HD, 256), BF16),
            VMEM((NZ, HD, 256), BF16),
            VMEM((ROWS, 128), F32),
            VMEM((ROWS, 128), F32),
            VMEM((ROWS, 256), BF16),
            VMEM((4 * share, D), BF16),
            VMEM((4 * share, D), BF16),
            VMEM((4 * share, D), F32),
            VMEM((6, share, D // 2), BF16),
            VMEM((6, share, D // 2), BF16),
            pltpu.SemaphoreType.DMA((16,)),
            pltpu.SemaphoreType.DMA((count,)),
            pltpu.SemaphoreType.DMA((count,)),
        ],
        compiler_params=pltpu.CompilerParams(
            collective_id=0, has_side_effects=True, vmem_limit_bytes=63 * 2**20
        ),
        name="layer",
    )(lam, hid, gain, up, base, shift, rate, wr, wa, out_gain, *weights)


def per_device(
    hidden_in,
    in_gain,
    receptance_weight,
    key_weight,
    value_weight,
    decay_down,
    decay_up,
    decay_base,
    decay_shift,
    learn_rate,
    query_pair,
    key_pair,
    value_pair,
    mix_lambda,
    out_recurrent,
    out_attention,
    out_gain,
):
    layer_out, sums = run_layer(
        mix_lambda,
        hidden_in,
        in_gain.reshape(1, D),
        decay_up,
        decay_base.reshape(1, 128),
        decay_shift,
        learn_rate.reshape(1, 128),
        out_recurrent,
        out_attention,
        out_gain.reshape(1, D),
        (
            receptance_weight,
            key_weight,
            value_weight,
            decay_down,
            query_pair.reshape(D, 128),
            key_pair.reshape(D, 128),
            value_pair.reshape(D, 128),
        ),
    )
    return layer_out, sums


def solution(mesh):
    split_mesh = Mesh(mesh.devices.reshape(NZ, NX, NY, NC), ("z", "x", "y", "c"))
    sp, tp = ("z", "x"), ("y", "c")
    placed = (
        P(sp, tp),
        P(),
        P(None, tp),
        P(None, tp),
        P(None, tp),
        P(),
        P(None, tp),
        P(tp),
        P(sp, tp),
        P(tp),
        P(None, tp, None),
        P(None, tp, None),
        P(None, tp, None),
        P(tp),
        P(tp, None),
        P(tp, None),
        P(),
    )
    return jax.shard_map(
        per_device,
        mesh=split_mesh,
        in_specs=placed,
        out_specs=(P((*sp, *tp), None), P(tp, None, sp)),
        check_vma=False,
    )
```

```python
import functools
import math

import jax
import jax.numpy as jnp
from jax import lax
from jax.experimental import pallas as pl
from jax.experimental.pallas import tpu as pltpu
from jax.sharding import Mesh
from jax.sharding import PartitionSpec as P

F32 = jnp.float32
BF16 = jnp.bfloat16
HD = 64
NZ, NX, NY, NC = 8, 4, 4, 2
ROWS = 384
HALF = ROWS // 2
D = 2048
FEAT = 256
CHUNK = 128
SUB = 32
DECAY_SCALE = math.exp(-0.5)
NORM_EPS = 1e-06
GROUP_EPS = 0.00064
HEAD_EPS = 1e-05
KEY_EPS = 1e-06
NEGATIVE = -1e30
TINY = 1e-37
LOG2E = 1.4426950408889634
LN2 = 0.6931471805599453
MESH = pl.DeviceIdType.MESH
VMEM = pltpu.VMEM
HIGHEST = lax.Precision.HIGHEST


def dot(a, b):
    return jnp.dot(a, b, preferred_element_type=F32)


def dot_nt(a, b):
    return lax.dot_general(a, b, (((1,), (1,)), ((), ())), preferred_element_type=F32)


def split(x):
    high = x.astype(BF16)
    return high, (x - high.astype(F32)).astype(BF16)


def fine_dot(a, b):
    a_high, a_low = split(a)
    b_high, b_low = split(b)
    both = dot(jnp.concatenate([a_high, a_low], 1), jnp.concatenate([b_high, b_high], 0))
    return both + dot(a_high, b_low)


def fine_dot_nt(a, b):
    a_high, a_low = split(a)
    b_high, b_low = split(b)
    both = dot_nt(jnp.concatenate([a_high, a_low], 1), jnp.concatenate([b_high, b_high], 1))
    return both + dot_nt(a_high, b_low)


def coarse_dot(a, b):
    return dot(a.astype(BF16), b.astype(BF16))


def remote(src, dst, send_sem, recv_sem, where):
    return pltpu.make_async_remote_copy(
        src_ref=src,
        dst_ref=dst,
        send_sem=send_sem,
        recv_sem=recv_sem,
        device_id=where,
        device_id_type=MESH,
    )


def greet(places):
    barrier = pltpu.get_barrier_semaphore()
    for place in places:
        pl.semaphore_signal(barrier, inc=1, device_id=place, device_id_type=MESH)
    pl.semaphore_wait(barrier, len(places))


def iota(shape, dim):
    return lax.broadcasted_iota(jnp.int32, shape, dim)


def by_head(x):
    first = lax.rem(iota(x.shape, 1), 128) < HD
    zero = jnp.zeros_like(x)
    return jnp.concatenate([jnp.where(first, x, zero), jnp.where(first, zero, x)], 0)


def same_head(shape):
    return (iota(shape, 0) < HD) == (lax.rem(iota(shape, 1), 128) < HD)


SIZES = ((1, 8), (8, 32), (32, 128))


def blocks_mask(small, large):
    row, col = iota((CHUNK, CHUNK), 0), iota((CHUNK, CHUNK), 1)
    return (lax.div(row, large) == lax.div(col, large)) & (lax.div(row, small) > lax.div(col, small))


def inverses(lowers):
    row, col = iota((CHUNK, CHUNK), 0), iota((CHUNK, CHUNK), 1)
    identity = jnp.where(row == col, 1.0, 0.0)
    found = None
    for small, large in SIZES:
        keep = blocks_mask(small, large)
        parts = [jnp.where(keep, lower, 0.0) for lower in lowers]
        if found is None:
            steps = parts
            found = [identity + part for part in parts]
        else:
            steps = [coarse_dot(f, part) for f, part in zip(found, parts)]
            found = [f + coarse_dot(s, f) for f, s in zip(found, steps)]
        reach = 2
        while reach * small < large:
            steps = [coarse_dot(s, s) for s in steps]
            found = [f + coarse_dot(s, f) for f, s in zip(found, steps)]
            reach *= 2
    return found


def all_terms(receptance, keys, values, decays, rate):
    count = ROWS // CHUNK
    cuts = [slice(n * CHUNK, (n + 1) * CHUNK) for n in range(count)]
    row, col = iota((CHUNK, CHUNK), 0), iota((CHUNK, CHUNK), 1)
    ones = (row >= col).astype(BF16)
    first = col < HD
    w = [decays[at, :] for at in cuts]
    r = [receptance[at, :].astype(F32) for at in cuts]
    k = [keys[at, :].astype(F32) for at in cuts]
    v = [values[at, :] for at in cuts]
    running = []
    for part in w:
        high = part.astype(BF16)
        rest = part - high.astype(F32)
        middle = rest.astype(BF16)
        lowest = (rest - middle.astype(F32)).astype(BF16)
        running.append(
            dot(jnp.concatenate([ones, ones], 1), jnp.concatenate([high, middle], 0))
            + dot(ones, lowest)
        )
    before = [a - b for a, b in zip(running, w)]
    ending = [a[CHUNK - 1 :, :] for a in running]
    unit = []
    for part in k:
        square = part * part
        one = jnp.sum(jnp.where(first, square, 0.0), axis=1, keepdims=True)
        two = jnp.sum(jnp.where(first, 0.0, square), axis=1, keepdims=True)
        unit.append(part * lax.rsqrt(jnp.where(first, one, two) + KEY_EPS))
    erasing = [u * rate for u in unit]
    pieces = [[] for _ in cuts]
    for i in range(CHUNK // SUB):
        at = slice(i * SUB, (i + 1) * SUB)
        for n in range(count):
            start = running[n][i * SUB - 1 : i * SUB, :] if i else jnp.zeros_like(ending[n])
            left = jnp.concatenate(
                [
                    -unit[n][at] * jnp.exp(before[n][at] - start),
                    r[n][at] * jnp.exp(running[n][at] - start),
                ],
                0,
            )
            growth = jnp.exp(jnp.where(row < (i + 1) * SUB, start - running[n], -100.0))
            right = jnp.concatenate([erasing[n] * growth, k[n] * growth], 0)
            pieces[n].append(fine_dot_nt(by_head(left), right))

    def matrix(n, head, read, which, keep):
        at = head * 2 * SUB + read * SUB
        whole = jnp.concatenate(
            [p[at : at + SUB, which * CHUNK : (which + 1) * CHUNK] for p in pieces[n]], 0
        )
        return jnp.where(keep, whole, 0.0)

    strict, causal = row > col, row >= col
    found = inverses([matrix(n, h, 0, 0, strict) for n in range(count) for h in range(2)])
    found = [jnp.concatenate(found[2 * n : 2 * n + 2], 1) for n in range(count)]

    def pair(n, read, which, keep):
        return jnp.concatenate(
            [matrix(n, h, read, which, keep).astype(BF16) for h in range(2)], 1
        )

    by_value = [by_head(part) for part in v]
    carried = [dot(pair(n, 0, 1, strict), by_value[n]) for n in range(count)]
    right_side = [
        by_head(jnp.concatenate([-unit[n] * jnp.exp(before[n]), carried[n]], 1))
        for n in range(count)
    ]
    solved = [fine_dot(found[n], right_side[n]) for n in range(count)]
    seen = [
        dot(pair(n, 1, 0, causal), by_head(solved[n].astype(BF16))) for n in range(count)
    ]
    local = [seen[n][:, 128:] + dot(pair(n, 1, 1, causal), by_value[n]) for n in range(count)]
    read_state = [r[n] * jnp.exp(running[n]) + seen[n][:, :128] for n in range(count)]
    none = jnp.zeros((CHUNK, 128), F32)
    wide_row, wide_col = iota((128, 256), 0), iota((128, 256), 1)
    steps = []
    for n in range(count):
        to_end = jnp.exp(ending[n] - running[n])
        left = jnp.concatenate(
            [jnp.transpose(erasing[n] * to_end), jnp.transpose(k[n] * to_end)], 1
        )
        right = jnp.concatenate(
            [solved[n], jnp.concatenate([none, v[n].astype(F32)], 1)], 0
        )
        step = jnp.where(same_head((128, 256)), fine_dot(left, right), 0.0)
        decayed = jnp.concatenate(
            [jnp.broadcast_to(jnp.exp(ending[n]), (128, 128)), none], 1
        )
        steps.append(step + jnp.where(wide_row == wide_col, decayed, 0.0))
    return read_state, local, steps


def device_terms(receptance, keys, values, decays, rate):
    read_state, local, steps = all_terms(receptance, keys, values, decays, rate)
    reads, reach = [read_state[0]], [local[0]]
    so_far = steps[0]
    for n in range(1, len(steps)):
        seen = fine_dot(read_state[n], so_far)
        reads.append(seen[:, :128])
        reach.append(local[n] + seen[:, 128:])
        so_far = compose(steps[n], so_far)
    return reads, reach, so_far


def compose(later, earlier):
    out = fine_dot(later[:, :128], earlier)
    none = jnp.zeros((128, 128), F32)
    return out + jnp.concatenate([none, later[:, 128:]], 1)


def packed(step):
    return step[:HD] + step[HD:]


def unpacked(step):
    both = jnp.concatenate([step, step], 0)
    return jnp.where(same_head((128, 256)), both, 0.0)


def packed_identity():
    row, col = iota((HD, 256), 0), iota((HD, 256), 1)
    return jnp.where((col < 128) & (lax.rem(col, HD) == row), 1.0, 0.0)


class Courier:
    def __init__(self, ssem, rsem):
        self.ssem, self.rsem, self.copies = ssem, rsem, []

    def send(self, src, dst, where):
        n = len(self.copies)
        copy = remote(src, dst, self.ssem.at[n], self.rsem.at[n], where)
        copy.start()
        self.copies.append(copy)
        return copy


def load_all(places, sems, first):
    loads = []
    for n, (src, dst) in enumerate(places):
        load = pltpu.make_async_copy(src, dst, sems.at[first + n])
        load.start()
        loads.append(load)
    return loads


def layer(
    lam_ref,
    hid_hbm,
    gain_hbm,
    up_hbm,
    base_hbm,
    shift_hbm,
    rate_hbm,
    wr_hbm,
    wa_hbm,
    out_gain_hbm,
    *rest,
):
    weights = rest[:7]
    out_ref, sums_ref = rest[7:9]
    (
        hbuf,
        wbuf,
        proj,
        sumsq,
        gain_ref,
        up_ref,
        base_ref,
        shift_ref,
        rate_ref,
        out_w,
        out_gain_ref,
        q_ref,
        k_ref,
        vt_ref,
        r_ref,
        rk_ref,
        rv_ref,
        ld_ref,
        kbuf,
        vbuf,
        qbuf,
        qwide,
        acc,
        top,
        low,
        osend,
        orecv,
        stsend,
        strecv,
        joined,
        weigh,
        gxsend,
        gxbuf,
        gzsend,
        gzbuf,
        reads,
        local,
        mix_ref,
        psend,
        precv,
        pair,
        hsend,
        hrecv,
        wsem,
        ssem,
        rsem,
    ) = rest[9:]
    z = lax.axis_index("z")
    x = lax.axis_index("x")
    y = lax.axis_index("y")
    c = lax.axis_index("c")
    other = 1 - c
    up, down, across = lax.rem(y + 1, NY), lax.rem(y + 3, NY), lax.rem(y + 2, NY)
    own = y * 2 + c
    loads = load_all([(hid_hbm, hbuf.at[own])], wsem, 0)
    places = [(w, wbuf.at[:, pl.ds(n * 128, 128)]) for n, w in enumerate(weights)]
    places += [
        (gain_hbm, gain_ref),
        (up_hbm, up_ref),
        (base_hbm, base_ref),
        (shift_hbm, shift_ref),
        (rate_hbm, rate_ref),
        (wr_hbm, out_w.at[pl.ds(0, 128)]),
        (wa_hbm, out_w.at[pl.ds(128, 128)]),
        (out_gain_hbm, out_gain_ref),
    ]
    loads += load_all(places, wsem, 1)
    to_up, to_down, to_other = {"y": up}, {"y": down}, {"c": other}
    z_up, z_down = {"z": lax.rem(z + 1, NZ)}, {"z": lax.rem(z + NZ - 1, NZ)}
    z_others = [{"z": lax.rem(z + n, NZ)} for n in range(1, NZ)]
    x_others = [lax.rem(x + n, NX) for n in range(1, NX)]
    greet([to_up, to_down, to_other, z_up, z_down] + [{"x": n} for n in x_others])
    courier = Courier(ssem, rsem)
    send = courier.send
    loads[0].wait()

    first, second = pl.ds(0, HALF), pl.ds(HALF, HALF)

    def share(number, part, where):
        block = hbuf.at[number]
        if part is not None:
            block = block.at[part]
        return send(block, block, where)

    below, above, far = down * 2 + c, up * 2 + c, across * 2 + c
    below_first = share(own, first, to_up)
    above_second = share(own, second, to_down)
    below_second = share(own, second, to_up)
    above_first = share(own, first, to_down)
    beside = share(own, None, to_other)
    for load in loads[1:]:
        load.wait()

    def add(number, fresh=False):
        block = hbuf.at[number]
        at = pl.multiple_of(number * FEAT, FEAT)
        w = wbuf[pl.ds(at, FEAT), :]
        gain = gain_ref[:, pl.ds(at, FEAT)]

        for t in range(ROWS // 128):
            rows = pl.ds(t * 128, 128)
            h = block[rows, :].astype(F32)
            squares = h[:, :128] * h[:, :128] + h[:, 128:] * h[:, 128:]
            product = dot((h * gain).astype(BF16), w)
            if fresh:
                sumsq[rows, :] = squares
                proj[rows, :] = product
            else:
                sumsq[rows, :] += squares
                proj[rows, :] += product

    add(own, True)
    beside.wait_recv()
    add(y * 2 + other)
    below_first.wait_recv()
    far_first = share(below, first, to_up)
    relays = [share(below, first, to_other)]
    above_second.wait_recv()
    far_second = share(above, second, to_down)
    relays.append(share(above, second, to_other))
    below_second.wait_recv()
    relays.append(share(below, second, to_other))
    above_first.wait_recv()
    relays.append(share(above, first, to_other))
    add(below)
    add(above)
    far_first.wait_recv()
    relays.append(share(far, first, to_other))
    far_second.wait_recv()
    relays.append(share(far, second, to_other))
    relays[0].wait_recv()
    relays[2].wait_recv()
    add(down * 2 + other)
    relays[1].wait_recv()
    relays[3].wait_recv()
    add(up * 2 + other)
    add(far)
    relays[4].wait_recv()
    relays[5].wait_recv()
    add(across * 2 + other)

    total = jnp.sum(sumsq[...], axis=1, keepdims=True)
    scale = lax.rsqrt(total * (1.0 / D) + NORM_EPS)
    k_ref[...] = (proj[:, 640:768] * scale).astype(BF16)
    vt_ref[...] = jnp.transpose(proj[:, 768:896] * scale).astype(BF16)
    q_ref[...] = (proj[:, 512:640] * (scale * (LOG2E * HD**-0.5))).astype(BF16)

    def pass_on(buf, source, slot, first, second):
        source[0].wait_recv()
        ahead = send(buf.at[slot - 1, first], buf.at[slot if slot < 3 else 6, first], z_up)
        source[1].wait_recv()
        back = send(buf.at[slot + 2, second], buf.at[slot + 3, second], z_down)
        return ahead, back

    key_all, value_all = pl.ds(0, ROWS), pl.ds(0, 128)
    keys = (send(k_ref, kbuf.at[0], z_up), send(k_ref, kbuf.at[3], z_down))
    values = (send(vt_ref, vbuf.at[0], z_up), send(vt_ref, vbuf.at[3], z_down))
    q_copies = [send(q_ref, qbuf.at[x], {"x": x_others[n]}) for n in (1, 0, 2)]

    @pl.loop(0, ROWS // 128)
    def _(t):
        rows = pl.ds(pl.multiple_of(t * 128, 128), 128)
        total = jnp.sum(sumsq[rows, :], axis=1, keepdims=True)
        scale = lax.rsqrt(total * (1.0 / D) + NORM_EPS)
        r_ref[rows, :] = (proj[rows, 0:128] * scale).astype(BF16)
        rk_ref[rows, :] = (proj[rows, 128:256] * scale).astype(BF16)
        rv_ref[rows, :] = (proj[rows, 256:384] * scale).astype(BF16)
        down_low = jnp.tanh(proj[rows, 384:512] * scale).astype(BF16)
        gate = dot(down_low, up_ref[...]) + base_ref[...]
        ld_ref[rows, :] = -DECAY_SCALE * jax.nn.sigmoid(gate) + shift_ref[rows, :]

    found_reads, found_local, so_far = device_terms(r_ref, rk_ref, rv_ref, ld_ref, rate_ref[...])
    for n in range(ROWS // CHUNK):
        reads[n * CHUNK : (n + 1) * CHUNK, :] = found_reads[n]
        local[n * CHUNK : (n + 1) * CHUNK, :] = found_local[n]
    gxsend[...] = packed(so_far)
    gxbuf[x] = packed(so_far)
    gx_copies = [send(gxsend, gxbuf.at[x], {"x": n}) for n in x_others]

    keys = pass_on(kbuf, keys, 1, key_all, key_all)
    values = pass_on(vbuf, values, 1, value_all, value_all)

    qbuf[x] = q_ref[...]
    for copy in q_copies:
        copy.wait_recv()
    for j in range(NX):
        qwide[j] = by_head(qbuf[j])
    tiles = [slice(t * 256, (t + 1) * 256) for t in range(3)]

    def attend_all(k_block, v_block, own):
        k_all, v_all = k_block[...], v_block[...]

        def scores_of(j):
            found = [dot_nt(k_all, qwide[j, cols, :]) for cols in tiles]
            if own:
                for t in range(3):
                    key_at = iota((ROWS, 256), 0)
                    query_at = lax.rem(iota((ROWS, 256), 1) + t * 256, ROWS)
                    keep = query_at - key_at >= (x - j) * ROWS
                    found[t] = jnp.where(keep, found[t], NEGATIVE)
            return found, [jnp.max(s, axis=0, keepdims=True) for s in found]

        ready = scores_of(0)
        for j in range(NX):
            following = scores_of(j + 1) if j + 1 < NX else None
            scores, highest = ready
            if not own:
                olds = [top[j, 0:1, cols] for cols in tiles]
                sums = [low[j, 0:1, cols] for cols in tiles]
                totals = [acc[j, :, cols] for cols in tiles]
            for t, cols in enumerate(tiles):
                new = highest[t] if own else jnp.maximum(olds[t], highest[t])
                weights = jnp.exp2(scores[t] - new)
                part = jnp.sum(weights, axis=0, keepdims=True)
                seen = dot(v_all, weights.astype(BF16))
                top[j, 0:1, cols] = new
                if own:
                    low[j, 0:1, cols] = part
                    acc[j, :, cols] = seen
                else:
                    rescale = jnp.exp2(olds[t] - new)
                    low[j, 0:1, cols] = sums[t] * rescale + part
                    acc[j, :, cols] = totals[t] * rescale + seen
            ready = following

    def attend(slot, needed):
        @pl.when(needed)
        def _():
            attend_all(kbuf.at[slot], vbuf.at[slot], False)

    attend_all(k_ref, vt_ref, True)
    keys = pass_on(kbuf, keys, 2, key_all, key_all)
    attend(0, z >= 1)
    values = pass_on(vbuf, values, 2, value_all, value_all)
    attend(3, z >= NZ - 1)

    for copy in gx_copies:
        copy.wait_recv()
    none = jnp.zeros((128, 128), F32)
    identity = jnp.where(iota((128, 256), 0) == iota((128, 256), 1), 1.0, 0.0)
    before_x = identity
    total = unpacked(gxbuf[0])
    for n in range(1, NX):
        before_x = jnp.where(x == n, total, before_x)
        total = compose(unpacked(gxbuf[n]), total)
    share = (packed(total) - packed_identity()).astype(BF16)
    gzsend[...] = share
    gzbuf[z] = share

    keys = pass_on(kbuf, keys, 3, pl.ds(0, HALF), pl.ds(HALF, HALF))
    attend(1, z >= 2)
    values = pass_on(vbuf, values, 3, pl.ds(0, HD), pl.ds(HD, HD))
    attend(4, z >= NZ - 2)
    attend(2, z >= 3)
    attend(5, z >= NZ - 3)
    for copy in (*keys, *values):
        copy.wait_recv()
    gz_copies = [send(gzsend, gzbuf.at[z], place) for place in z_others]
    attend(6, z >= 4)

    totals = jnp.maximum(jnp.concatenate([low[j, 0:1, :] for j in range(NX)], 0), TINY)
    level = jnp.concatenate([top[j, 0:1, :] for j in range(NX)], 0) + jnp.log2(totals)
    stsend[...] = level
    st_copies = [send(stsend, strecv.at[n], {"x": x_others[n]}) for n in (1, 0, 2)]
    for copy in st_copies:
        copy.wait_recv()
    theirs = [strecv[n] for n in range(3)]
    highest = functools.reduce(jnp.maximum, theirs, level)
    whole = sum((jnp.exp2(one - highest) for one in theirs), jnp.exp2(level - highest))
    joint = highest + jnp.log2(whole)
    joined[...] = joint
    weigh[...] = jnp.exp2(level - joint) / totals

    def contribution(j):
        w = weigh[pl.ds(j, 1), :]
        part = acc[j]
        return part[:, :ROWS] * w[:, :ROWS] - part[:, ROWS:] * (lam_ref[0] * w[:, ROWS:])

    o_copies = []
    for n in (1, 0, 2):
        osend[n] = contribution(x_others[n]).astype(BF16)
        o_copies.append(send(osend.at[n], orecv.at[n], {"x": x_others[n]}))
    head_out = contribution(x)
    sums = joined[pl.ds(x, 1), :] * LN2
    sums_ref[0, 0:1, :] = sums[:, :ROWS]
    sums_ref[0, 1:2, :] = sums[:, ROWS:]

    for copy in gz_copies:
        copy.wait_recv()
    state = none
    for n in range(NZ - 1):
        step = unpacked(gzbuf[n].astype(F32) + packed_identity())
        after = fine_dot(step[:, :128], state) + step[:, 128:]
        state = jnp.where(n < z, after, state)
    state = fine_dot(before_x[:, :128], state) + before_x[:, 128:]
    recurrent = local[...] + fine_dot(reads[...], state)
    first = iota((ROWS, 128), 1) < HD

    def head_mean(values):
        one = jnp.sum(jnp.where(first, values, 0.0), axis=1, keepdims=True)
        two = jnp.sum(jnp.where(first, 0.0, values), axis=1, keepdims=True)
        return jnp.where(first, one, two) * (1.0 / HD)

    centered = recurrent - head_mean(recurrent)
    normal = centered * lax.rsqrt(head_mean(centered * centered) + GROUP_EPS)
    mix_ref[:, 0:128] = normal.astype(BF16)

    for copy in o_copies:
        copy.wait_recv()
    for n in range(3):
        head_out = head_out + orecv[n].astype(F32)
    head_out = head_out * lax.rsqrt(
        jnp.mean(head_out * head_out, axis=0, keepdims=True) + HEAD_EPS
    )
    mix_ref[:, 128:256] = jnp.transpose(head_out).astype(BF16)

    part_rows = ROWS // (NY * NC)
    order = [across, up, down, y]

    def rows_for(core):
        return jnp.concatenate(
            [
                mix_ref[pl.ds(pl.multiple_of((n * 2 + core) * part_rows, part_rows), part_rows), :]
                for n in order
            ],
            0,
        )

    theirs = rows_for(other)
    ours = rows_for(c)
    for t in range(8):
        cols = slice(t * 256, (t + 1) * 256)
        psend[:, cols] = dot(theirs, out_w[:, cols]).astype(BF16)
    pairs = [
        send(psend.at[pl.ds(n * part_rows, part_rows)], precv.at[pl.ds(n * part_rows, part_rows)], to_other)
        for n in range(4)
    ]
    for t in range(8):
        cols = slice(t * 256, (t + 1) * 256)
        pair[:, cols] = dot(ours, out_w[:, cols])
    one, two = slice(0, D // 2), slice(D // 2, D)

    def summed(n, half):
        at = slice(n * part_rows, (n + 1) * part_rows)
        return pair[at, half] + precv[at, half].astype(F32)

    pairs[0].wait_recv()
    hsend[0] = summed(0, one).astype(BF16)
    relay_up = send(hsend.at[0], hrecv.at[0], to_up)
    hsend[1] = summed(0, two).astype(BF16)
    relay_down = send(hsend.at[1], hrecv.at[1], to_down)
    pairs[1].wait_recv()
    hsend[2] = summed(1, two).astype(BF16)
    plain_up = send(hsend.at[2], hrecv.at[2], to_up)
    pairs[2].wait_recv()
    hsend[3] = summed(2, one).astype(BF16)
    plain_down = send(hsend.at[3], hrecv.at[3], to_down)
    relay_up.wait_recv()
    hsend[4] = (summed(1, one) + hrecv[0].astype(F32)).astype(BF16)
    merged_up = send(hsend.at[4], hrecv.at[4], to_up)
    relay_down.wait_recv()
    hsend[5] = (summed(2, two) + hrecv[1].astype(F32)).astype(BF16)
    merged_down = send(hsend.at[5], hrecv.at[5], to_down)
    pairs[3].wait_recv()
    plain_up.wait_recv()
    plain_down.wait_recv()
    left_half = summed(3, one) + hrecv[3].astype(F32)
    right_half = summed(3, two) + hrecv[2].astype(F32)
    merged_up.wait_recv()
    merged_down.wait_recv()
    left_half = left_half + hrecv[4].astype(F32)
    right_half = right_half + hrecv[5].astype(F32)
    total = jnp.sum(left_half * left_half, axis=1, keepdims=True) + jnp.sum(
        right_half * right_half, axis=1, keepdims=True
    )
    scale = lax.rsqrt(total * (1.0 / D) + NORM_EPS)
    out_ref[:, one] = (left_half * scale * out_gain_ref[:, one]).astype(BF16)
    out_ref[:, two] = (right_half * scale * out_gain_ref[:, two]).astype(BF16)
    for copy in courier.copies:
        copy.wait_send()


def run_layer(lam, hid, gain, up, base, shift, rate, wr, wa, out_gain, weights):
    whole = pl.BlockSpec(memory_space=VMEM)
    far = pl.BlockSpec(memory_space=pl.ANY)
    share = ROWS // (NY * NC)
    count = 13 + 16 + 3 + 3 + 7 + 6 + 10
    rows = VMEM((ROWS, 128), BF16)
    return pl.pallas_call(
        layer,
        out_shape=(
            jax.ShapeDtypeStruct((share, D), BF16),
            jax.ShapeDtypeStruct((1, 2, ROWS), F32),
        ),
        in_specs=[pl.BlockSpec(memory_space=pltpu.SMEM)] + [far] * 16,
        out_specs=(whole, whole),
        scratch_shapes=[
            VMEM((NY * NC, ROWS, FEAT), BF16),
            VMEM((D, 896), BF16),
            VMEM((ROWS, 896), F32),
            VMEM((ROWS, 128), F32),
            VMEM((1, D), F32),
            VMEM((128, 128), BF16),
            VMEM((1, 128), F32),
            VMEM((ROWS, 128), F32),
            VMEM((1, 128), F32),
            VMEM((256, D), BF16),
            VMEM((1, D), F32),
            rows,
            rows,
            VMEM((128, ROWS), BF16),
            rows,
            rows,
            rows,
            VMEM((ROWS, 128), F32),
            VMEM((7, ROWS, 128), BF16),
            VMEM((7, 128, ROWS), BF16),
            VMEM((NX, ROWS, 128), BF16),
            VMEM((NX, 2 * ROWS, 128), BF16),
            VMEM((NX, 128, 2 * ROWS), F32),
            VMEM((NX, 8, 2 * ROWS), F32),
            VMEM((NX, 8, 2 * ROWS), F32),
            VMEM((3, 128, ROWS), BF16),
            VMEM((3, 128, ROWS), BF16),
            VMEM((NX, 2 * ROWS), F32),
            VMEM((3, NX, 2 * ROWS), F32),
            VMEM((NX, 2 * ROWS), F32),
            VMEM((NX, 2 * ROWS), F32),
            VMEM((HD, 256), F32),
            VMEM((NX, HD, 256), F32),
            VMEM((HD, 256), BF16),
            VMEM((NZ, HD, 256), BF16),
            VMEM((ROWS, 128), F32),
            VMEM((ROWS, 128), F32),
            VMEM((ROWS, 256), BF16),
            VMEM((4 * share, D), BF16),
            VMEM((4 * share, D), BF16),
            VMEM((4 * share, D), F32),
            VMEM((6, share, D // 2), BF16),
            VMEM((6, share, D // 2), BF16),
            pltpu.SemaphoreType.DMA((16,)),
            pltpu.SemaphoreType.DMA((count,)),
            pltpu.SemaphoreType.DMA((count,)),
        ],
        compiler_params=pltpu.CompilerParams(
            collective_id=0, has_side_effects=True, vmem_limit_bytes=63 * 2**20
        ),
        name="layer",
    )(lam, hid, gain, up, base, shift, rate, wr, wa, out_gain, *weights)


def per_device(
    hidden_in,
    in_gain,
    receptance_weight,
    key_weight,
    value_weight,
    decay_down,
    decay_up,
    decay_base,
    decay_shift,
    learn_rate,
    query_pair,
    key_pair,
    value_pair,
    mix_lambda,
    out_recurrent,
    out_attention,
    out_gain,
):
    layer_out, sums = run_layer(
        mix_lambda,
        hidden_in,
        in_gain.reshape(1, D),
        decay_up,
        decay_base.reshape(1, 128),
        decay_shift,
        learn_rate.reshape(1, 128),
        out_recurrent,
        out_attention,
        out_gain.reshape(1, D),
        (
            receptance_weight,
            key_weight,
            value_weight,
            decay_down,
            query_pair.reshape(D, 128),
            key_pair.reshape(D, 128),
            value_pair.reshape(D, 128),
        ),
    )
    return layer_out, sums


def solution(mesh):
    split_mesh = Mesh(mesh.devices.reshape(NZ, NX, NY, NC), ("z", "x", "y", "c"))
    sp, tp = ("z", "x"), ("y", "c")
    placed = (
        P(sp, tp),
        P(),
        P(None, tp),
        P(None, tp),
        P(None, tp),
        P(),
        P(None, tp),
        P(tp),
        P(sp, tp),
        P(tp),
        P(None, tp, None),
        P(None, tp, None),
        P(None, tp, None),
        P(tp),
        P(tp, None),
        P(tp, None),
        P(),
    )
    return jax.shard_map(
        per_device,
        mesh=split_mesh,
        in_specs=placed,
        out_specs=(P((*sp, *tp), None), P(tp, None, sp)),
        check_vma=False,
    )
```

```python
import functools
import math

import jax
import jax.numpy as jnp
from jax import lax
from jax.experimental import pallas as pl
from jax.experimental.pallas import tpu as pltpu
from jax.sharding import Mesh
from jax.sharding import PartitionSpec as P

F32 = jnp.float32
BF16 = jnp.bfloat16
HD = 64
NZ, NX, NY, NC = 8, 4, 4, 2
ROWS = 384
HALF = ROWS // 2
D = 2048
FEAT = 256
CHUNK = 128
SUB = 32
DECAY_SCALE = math.exp(-0.5)
NORM_EPS = 1e-06
GROUP_EPS = 0.00064
HEAD_EPS = 1e-05
KEY_EPS = 1e-06
NEGATIVE = -1e30
TINY = 1e-37
LOG2E = 1.4426950408889634
LN2 = 0.6931471805599453
MESH = pl.DeviceIdType.MESH
VMEM = pltpu.VMEM
HIGHEST = lax.Precision.HIGHEST


def dot(a, b):
    return jnp.dot(a, b, preferred_element_type=F32)


def dot_nt(a, b):
    return lax.dot_general(a, b, (((1,), (1,)), ((), ())), preferred_element_type=F32)


def split(x):
    high = x.astype(BF16)
    return high, (x - high.astype(F32)).astype(BF16)


def fine_dot(a, b):
    a_high, a_low = split(a)
    b_high, b_low = split(b)
    both = dot(jnp.concatenate([a_high, a_low], 1), jnp.concatenate([b_high, b_high], 0))
    return both + dot(a_high, b_low)


def fine_dot_nt(a, b):
    a_high, a_low = split(a)
    b_high, b_low = split(b)
    both = dot_nt(jnp.concatenate([a_high, a_low], 1), jnp.concatenate([b_high, b_high], 1))
    return both + dot_nt(a_high, b_low)


def coarse_dot(a, b):
    return dot(a.astype(BF16), b.astype(BF16))


def remote(src, dst, send_sem, recv_sem, where):
    return pltpu.make_async_remote_copy(
        src_ref=src,
        dst_ref=dst,
        send_sem=send_sem,
        recv_sem=recv_sem,
        device_id=where,
        device_id_type=MESH,
    )


def greet(places):
    barrier = pltpu.get_barrier_semaphore()
    for place in places:
        pl.semaphore_signal(barrier, inc=1, device_id=place, device_id_type=MESH)
    pl.semaphore_wait(barrier, len(places))


def iota(shape, dim):
    return lax.broadcasted_iota(jnp.int32, shape, dim)


def by_head(x):
    first = lax.rem(iota(x.shape, 1), 128) < HD
    zero = jnp.zeros_like(x)
    return jnp.concatenate([jnp.where(first, x, zero), jnp.where(first, zero, x)], 0)


def same_head(shape):
    return (iota(shape, 0) < HD) == (lax.rem(iota(shape, 1), 128) < HD)


SIZES = ((1, 8), (8, 32), (32, 128))


def blocks_mask(small, large):
    row, col = iota((CHUNK, CHUNK), 0), iota((CHUNK, CHUNK), 1)
    return (lax.div(row, large) == lax.div(col, large)) & (lax.div(row, small) > lax.div(col, small))


def inverses(lowers):
    row, col = iota((CHUNK, CHUNK), 0), iota((CHUNK, CHUNK), 1)
    identity = jnp.where(row == col, 1.0, 0.0)
    found = None
    for small, large in SIZES:
        keep = blocks_mask(small, large)
        parts = [jnp.where(keep, lower, 0.0) for lower in lowers]
        if found is None:
            steps = parts
            found = [identity + part for part in parts]
        else:
            steps = [coarse_dot(f, part) for f, part in zip(found, parts)]
            found = [f + coarse_dot(s, f) for f, s in zip(found, steps)]
        reach = 2
        while reach * small < large:
            steps = [coarse_dot(s, s) for s in steps]
            found = [f + coarse_dot(s, f) for f, s in zip(found, steps)]
            reach *= 2
    return found


def all_terms(receptance, keys, values, decays, rate):
    count = ROWS // CHUNK
    cuts = [slice(n * CHUNK, (n + 1) * CHUNK) for n in range(count)]
    row, col = iota((CHUNK, CHUNK), 0), iota((CHUNK, CHUNK), 1)
    ones = (row >= col).astype(BF16)
    first = col < HD
    w = [decays[at, :] for at in cuts]
    r = [receptance[at, :].astype(F32) for at in cuts]
    k = [keys[at, :].astype(F32) for at in cuts]
    v = [values[at, :] for at in cuts]
    running = []
    for part in w:
        high = part.astype(BF16)
        rest = part - high.astype(F32)
        middle = rest.astype(BF16)
        lowest = (rest - middle.astype(F32)).astype(BF16)
        running.append(
            dot(jnp.concatenate([ones, ones], 1), jnp.concatenate([high, middle], 0))
            + dot(ones, lowest)
        )
    before = [a - b for a, b in zip(running, w)]
    ending = [a[CHUNK - 1 :, :] for a in running]
    unit = []
    for part in k:
        square = part * part
        one = jnp.sum(jnp.where(first, square, 0.0), axis=1, keepdims=True)
        two = jnp.sum(jnp.where(first, 0.0, square), axis=1, keepdims=True)
        unit.append(part * lax.rsqrt(jnp.where(first, one, two) + KEY_EPS))
    erasing = [u * rate for u in unit]
    pieces = [[] for _ in cuts]
    for i in range(CHUNK // SUB):
        at = slice(i * SUB, (i + 1) * SUB)
        for n in range(count):
            start = running[n][i * SUB - 1 : i * SUB, :] if i else jnp.zeros_like(ending[n])
            left = jnp.concatenate(
                [
                    -unit[n][at] * jnp.exp(before[n][at] - start),
                    r[n][at] * jnp.exp(running[n][at] - start),
                ],
                0,
            )
            growth = jnp.exp(jnp.where(row < (i + 1) * SUB, start - running[n], -100.0))
            right = jnp.concatenate([erasing[n] * growth, k[n] * growth], 0)
            pieces[n].append(fine_dot_nt(by_head(left), right))

    def matrix(n, head, read, which, keep):
        at = head * 2 * SUB + read * SUB
        whole = jnp.concatenate(
            [p[at : at + SUB, which * CHUNK : (which + 1) * CHUNK] for p in pieces[n]], 0
        )
        return jnp.where(keep, whole, 0.0)

    strict, causal = row > col, row >= col
    found = inverses([matrix(n, h, 0, 0, strict) for n in range(count) for h in range(2)])
    found = [jnp.concatenate(found[2 * n : 2 * n + 2], 1) for n in range(count)]

    def pair(n, read, which, keep):
        return jnp.concatenate(
            [matrix(n, h, read, which, keep).astype(BF16) for h in range(2)], 1
        )

    by_value = [by_head(part) for part in v]
    carried = [dot(pair(n, 0, 1, strict), by_value[n]) for n in range(count)]
    right_side = [
        by_head(jnp.concatenate([-unit[n] * jnp.exp(before[n]), carried[n]], 1))
        for n in range(count)
    ]
    solved = [fine_dot(found[n], right_side[n]) for n in range(count)]
    seen = [
        dot(pair(n, 1, 0, causal), by_head(solved[n].astype(BF16))) for n in range(count)
    ]
    local = [seen[n][:, 128:] + dot(pair(n, 1, 1, causal), by_value[n]) for n in range(count)]
    read_state = [r[n] * jnp.exp(running[n]) + seen[n][:, :128] for n in range(count)]
    none = jnp.zeros((CHUNK, 128), F32)
    wide_row, wide_col = iota((128, 256), 0), iota((128, 256), 1)
    steps = []
    for n in range(count):
        to_end = jnp.exp(ending[n] - running[n])
        left = jnp.concatenate(
            [jnp.transpose(erasing[n] * to_end), jnp.transpose(k[n] * to_end)], 1
        )
        right = jnp.concatenate(
            [solved[n], jnp.concatenate([none, v[n].astype(F32)], 1)], 0
        )
        step = jnp.where(same_head((128, 256)), fine_dot(left, right), 0.0)
        decayed = jnp.concatenate(
            [jnp.broadcast_to(jnp.exp(ending[n]), (128, 128)), none], 1
        )
        steps.append(step + jnp.where(wide_row == wide_col, decayed, 0.0))
    return read_state, local, steps


def device_terms(receptance, keys, values, decays, rate):
    read_state, local, steps = all_terms(receptance, keys, values, decays, rate)
    reads, reach = [read_state[0]], [local[0]]
    so_far = steps[0]
    for n in range(1, len(steps)):
        seen = fine_dot(read_state[n], so_far)
        reads.append(seen[:, :128])
        reach.append(local[n] + seen[:, 128:])
        so_far = compose(steps[n], so_far)
    return reads, reach, so_far


def compose(later, earlier):
    out = fine_dot(later[:, :128], earlier)
    none = jnp.zeros((128, 128), F32)
    return out + jnp.concatenate([none, later[:, 128:]], 1)


def packed(step):
    return step[:HD] + step[HD:]


def unpacked(step):
    both = jnp.concatenate([step, step], 0)
    return jnp.where(same_head((128, 256)), both, 0.0)


def packed_identity():
    row, col = iota((HD, 256), 0), iota((HD, 256), 1)
    return jnp.where((col < 128) & (lax.rem(col, HD) == row), 1.0, 0.0)


class Courier:
    def __init__(self, ssem, rsem):
        self.ssem, self.rsem, self.copies = ssem, rsem, []

    def make(self, src, dst, where):
        n = len(self.copies)
        copy = remote(src, dst, self.ssem.at[n], self.rsem.at[n], where)
        self.copies.append(copy)
        return copy

    def send(self, src, dst, where):
        copy = self.make(src, dst, where)
        copy.start()
        return copy


def load_all(places, sems, first):
    loads = []
    for n, (src, dst) in enumerate(places):
        load = pltpu.make_async_copy(src, dst, sems.at[first + n])
        load.start()
        loads.append(load)
    return loads


def layer(
    lam_ref,
    hid_hbm,
    gain_hbm,
    up_hbm,
    base_hbm,
    shift_hbm,
    rate_hbm,
    wr_hbm,
    wa_hbm,
    out_gain_hbm,
    *rest,
):
    weights = rest[:7]
    out_ref, sums_ref = rest[7:9]
    (
        hbuf,
        wbuf,
        proj,
        sumsq,
        gain_ref,
        up_ref,
        base_ref,
        shift_ref,
        rate_ref,
        out_w,
        out_gain_ref,
        q_ref,
        k_ref,
        vt_ref,
        r_ref,
        rk_ref,
        rv_ref,
        ld_ref,
        kbuf,
        vbuf,
        qbuf,
        qwide,
        acc,
        top,
        low,
        osend,
        orecv,
        stsend,
        strecv,
        joined,
        weigh,
        gxsend,
        gxbuf,
        gzsend,
        gzbuf,
        reads,
        local,
        state_ref,
        mix_ref,
        psend,
        precv,
        pair,
        hsend,
        hrecv,
        wsem,
        ssem,
        rsem,
    ) = rest[9:]
    z = lax.axis_index("z")
    x = lax.axis_index("x")
    y = lax.axis_index("y")
    c = lax.axis_index("c")
    other = 1 - c
    up, down, across = lax.rem(y + 1, NY), lax.rem(y + 3, NY), lax.rem(y + 2, NY)
    own = y * 2 + c
    loads = load_all([(hid_hbm, hbuf.at[own])], wsem, 0)
    places = [(w, wbuf.at[:, pl.ds(n * 128, 128)]) for n, w in enumerate(weights)]
    places += [
        (gain_hbm, gain_ref),
        (up_hbm, up_ref),
        (base_hbm, base_ref),
        (shift_hbm, shift_ref),
        (rate_hbm, rate_ref),
        (wr_hbm, out_w.at[pl.ds(0, 128)]),
        (wa_hbm, out_w.at[pl.ds(128, 128)]),
        (out_gain_hbm, out_gain_ref),
    ]
    loads += load_all(places, wsem, 1)
    to_up, to_down, to_other = {"y": up}, {"y": down}, {"c": other}
    z_up, z_down = {"z": lax.rem(z + 1, NZ)}, {"z": lax.rem(z + NZ - 1, NZ)}
    z_others = [{"z": lax.rem(z + n, NZ)} for n in range(1, NZ)]
    x_others = [lax.rem(x + n, NX) for n in range(1, NX)]
    greet([to_up, to_down, to_other, z_up, z_down] + [{"x": n} for n in x_others])
    courier = Courier(ssem, rsem)
    send = courier.send
    loads[0].wait()

    first, second = pl.ds(0, HALF), pl.ds(HALF, HALF)

    def share(number, part, where):
        block = hbuf.at[number]
        if part is not None:
            block = block.at[part]
        return send(block, block, where)

    below, above, far = down * 2 + c, up * 2 + c, across * 2 + c
    below_first = share(own, first, to_up)
    above_second = share(own, second, to_down)
    below_second = share(own, second, to_up)
    above_first = share(own, first, to_down)
    beside = share(own, None, to_other)
    for load in loads[1:]:
        load.wait()

    def add(number, fresh=False):
        block = hbuf.at[number]
        at = pl.multiple_of(number * FEAT, FEAT)
        w = wbuf[pl.ds(at, FEAT), :]
        gain = gain_ref[:, pl.ds(at, FEAT)]

        for t in range(ROWS // 128):
            rows = pl.ds(t * 128, 128)
            h = block[rows, :].astype(F32)
            squares = h[:, :128] * h[:, :128] + h[:, 128:] * h[:, 128:]
            product = dot((h * gain).astype(BF16), w)
            if fresh:
                sumsq[rows, :] = squares
                proj[rows, :] = product
            else:
                sumsq[rows, :] += squares
                proj[rows, :] += product

    add(own, True)
    beside.wait_recv()
    add(y * 2 + other)
    below_first.wait_recv()
    far_first = share(below, first, to_up)
    relays = [share(below, first, to_other)]
    above_second.wait_recv()
    far_second = share(above, second, to_down)
    relays.append(share(above, second, to_other))
    below_second.wait_recv()
    relays.append(share(below, second, to_other))
    above_first.wait_recv()
    relays.append(share(above, first, to_other))
    add(below)
    add(above)
    far_first.wait_recv()
    relays.append(share(far, first, to_other))
    far_second.wait_recv()
    relays.append(share(far, second, to_other))
    relays[0].wait_recv()
    relays[2].wait_recv()
    add(down * 2 + other)
    relays[1].wait_recv()
    relays[3].wait_recv()
    add(up * 2 + other)
    add(far)
    relays[4].wait_recv()
    relays[5].wait_recv()
    add(across * 2 + other)

    total = jnp.sum(sumsq[...], axis=1, keepdims=True)
    scale = lax.rsqrt(total * (1.0 / D) + NORM_EPS)
    k_ref[...] = (proj[:, 640:768] * scale).astype(BF16)
    vt_ref[...] = jnp.transpose(proj[:, 768:896] * scale).astype(BF16)
    q_ref[...] = (proj[:, 512:640] * (scale * (LOG2E * HD**-0.5))).astype(BF16)

    def pass_on(buf, source, slot, first, second):
        ahead = courier.make(
            buf.at[slot - 1, first], buf.at[slot if slot < 3 else 6, first], z_up
        )
        back = courier.make(buf.at[slot + 2, second], buf.at[slot + 3, second], z_down)

        def forth(n, copy):
            source[n].wait_recv()
            copy.start()

        @pl.when(z < 3)
        def _():
            forth(1, back)
            forth(0, ahead)

        @pl.when(z >= 3)
        def _():
            forth(0, ahead)
            forth(1, back)

        return ahead, back

    key_all, value_all = pl.ds(0, ROWS), pl.ds(0, 128)
    keys = (send(k_ref, kbuf.at[0], z_up), send(k_ref, kbuf.at[3], z_down))
    values = (send(vt_ref, vbuf.at[0], z_up), send(vt_ref, vbuf.at[3], z_down))
    q_copies = [send(q_ref, qbuf.at[x], {"x": x_others[n]}) for n in (1, 0, 2)]

    @pl.loop(0, ROWS // 128)
    def _(t):
        rows = pl.ds(pl.multiple_of(t * 128, 128), 128)
        total = jnp.sum(sumsq[rows, :], axis=1, keepdims=True)
        scale = lax.rsqrt(total * (1.0 / D) + NORM_EPS)
        r_ref[rows, :] = (proj[rows, 0:128] * scale).astype(BF16)
        rk_ref[rows, :] = (proj[rows, 128:256] * scale).astype(BF16)
        rv_ref[rows, :] = (proj[rows, 256:384] * scale).astype(BF16)
        down_low = jnp.tanh(proj[rows, 384:512] * scale).astype(BF16)
        gate = dot(down_low, up_ref[...]) + base_ref[...]
        ld_ref[rows, :] = -DECAY_SCALE * jax.nn.sigmoid(gate) + shift_ref[rows, :]

    found_reads, found_local, so_far = device_terms(r_ref, rk_ref, rv_ref, ld_ref, rate_ref[...])
    for n in range(ROWS // CHUNK):
        reads[n * CHUNK : (n + 1) * CHUNK, :] = found_reads[n]
        local[n * CHUNK : (n + 1) * CHUNK, :] = found_local[n]
    gxsend[...] = packed(so_far)
    gxbuf[x] = packed(so_far)
    gx_copies = [send(gxsend, gxbuf.at[x], {"x": n}) for n in x_others]

    keys = pass_on(kbuf, keys, 1, key_all, key_all)
    values = pass_on(vbuf, values, 1, value_all, value_all)

    qbuf[x] = q_ref[...]
    for copy in q_copies:
        copy.wait_recv()
    for j in range(NX):
        qwide[j] = by_head(qbuf[j])
    tiles = [slice(t * 256, (t + 1) * 256) for t in range(3)]

    def attend_all(blocks, own):
        k_all = [k_block[...] for k_block, _ in blocks]
        v_all = jnp.concatenate([v_block[...] for _, v_block in blocks], 1)

        def scores_of(j):
            found = [[dot_nt(k, qwide[j, cols, :]) for k in k_all] for cols in tiles]
            if own:
                for t in range(3):
                    key_at = iota((ROWS, 256), 0)
                    query_at = lax.rem(iota((ROWS, 256), 1) + t * 256, ROWS)
                    keep = query_at - key_at >= (x - j) * ROWS
                    found[t] = [jnp.where(keep, s, NEGATIVE) for s in found[t]]
            return found, [
                functools.reduce(
                    jnp.maximum, [jnp.max(s, axis=0, keepdims=True) for s in group]
                )
                for group in found
            ]

        ready = scores_of(0)
        for j in range(NX):
            following = scores_of(j + 1) if j + 1 < NX else None
            scores, highest = ready
            if not own:
                olds = [top[j, 0:1, cols] for cols in tiles]
                sums = [low[j, 0:1, cols] for cols in tiles]
                totals = [acc[j, :, cols] for cols in tiles]
            for t, cols in enumerate(tiles):
                new = highest[t] if own else jnp.maximum(olds[t], highest[t])
                weights = [jnp.exp2(s - new) for s in scores[t]]
                part = sum(jnp.sum(w, axis=0, keepdims=True) for w in weights)
                seen = dot(v_all, jnp.concatenate([w.astype(BF16) for w in weights], 0))
                top[j, 0:1, cols] = new
                if own:
                    low[j, 0:1, cols] = part
                    acc[j, :, cols] = seen
                else:
                    rescale = jnp.exp2(olds[t] - new)
                    low[j, 0:1, cols] = sums[t] * rescale + part
                    acc[j, :, cols] = totals[t] * rescale + seen
            ready = following

    def attend(slots, needed):
        @pl.when(needed)
        def _():
            attend_all([(kbuf.at[slot], vbuf.at[slot]) for slot in slots], False)

    attend_all([(k_ref, vt_ref)], True)
    keys = pass_on(kbuf, keys, 2, key_all, key_all)
    attend([0, 3], z == NZ - 1)
    attend([0], (z >= 1) & (z < NZ - 1))
    values = pass_on(vbuf, values, 2, value_all, value_all)

    for copy in gx_copies:
        copy.wait_recv()
    none = jnp.zeros((128, 128), F32)
    identity = jnp.where(iota((128, 256), 0) == iota((128, 256), 1), 1.0, 0.0)
    before_x = identity
    total = unpacked(gxbuf[0])
    for n in range(1, NX):
        before_x = jnp.where(x == n, total, before_x)
        total = compose(unpacked(gxbuf[n]), total)
    share = (packed(total) - packed_identity()).astype(BF16)
    gzsend[...] = share
    gzbuf[z] = share

    keys = pass_on(kbuf, keys, 3, pl.ds(0, HALF), pl.ds(HALF, HALF))
    attend([1, 4], z >= NZ - 2)
    attend([1], (z >= 2) & (z < NZ - 2))
    values = pass_on(vbuf, values, 3, pl.ds(0, HD), pl.ds(HD, HD))
    attend([2, 5], z >= NZ - 3)
    attend([2], (z >= 3) & (z < NZ - 3))
    gz_copies = []
    for n in range(1, NZ):
        at = 50 + n
        gz_copies.append(
            remote(gzsend, gzbuf.at[z], ssem.at[at], rsem.at[at], {"z": lax.rem(z + n, NZ)})
        )

    def finish_ring():
        for copy in (*keys, *values):
            copy.wait_recv()
        for n in range(1, NZ):

            @pl.when(z + n < NZ)
            def _(n=n):
                gz_copies[n - 1].start()

    @pl.when(z >= 4)
    def _():
        finish_ring()
        attend_all([(kbuf.at[6], vbuf.at[6])], False)

    totals = jnp.maximum(jnp.concatenate([low[j, 0:1, :] for j in range(NX)], 0), TINY)
    level = jnp.concatenate([top[j, 0:1, :] for j in range(NX)], 0) + jnp.log2(totals)
    stsend[...] = level
    st_copies = [send(stsend, strecv.at[n], {"x": x_others[n]}) for n in (1, 0, 2)]

    @pl.when(z < 4)
    def _():
        finish_ring()

    for copy in st_copies:
        copy.wait_recv()
    theirs = [strecv[n] for n in range(3)]
    highest = functools.reduce(jnp.maximum, theirs, level)
    whole = sum((jnp.exp2(one - highest) for one in theirs), jnp.exp2(level - highest))
    joint = highest + jnp.log2(whole)
    joined[...] = joint
    weigh[...] = jnp.exp2(level - joint) / totals

    def contribution(j):
        w = weigh[pl.ds(j, 1), :]
        part = acc[j]
        return part[:, :ROWS] * w[:, :ROWS] - part[:, ROWS:] * (lam_ref[0] * w[:, ROWS:])

    o_copies = []
    for n in (1, 0, 2):
        osend[n] = contribution(x_others[n]).astype(BF16)
        o_copies.append(send(osend.at[n], orecv.at[n], {"x": x_others[n]}))
    head_out = contribution(x)
    sums = joined[pl.ds(x, 1), :] * LN2
    sums_ref[0, 0:1, :] = sums[:, :ROWS]
    sums_ref[0, 1:2, :] = sums[:, ROWS:]

    for n in range(1, NZ):

        @pl.when(z >= n)
        def _(n=n):
            gz_copies[n - 1].wait_recv()

    state_ref[...] = none
    for n in range(NZ - 1):

        @pl.when(n < z)
        def _(n=n):
            step = unpacked(gzbuf[n].astype(F32) + packed_identity())
            state_ref[...] = fine_dot(step[:, :128], state_ref[...]) + step[:, 128:]

    state = fine_dot(before_x[:, :128], state_ref[...]) + before_x[:, 128:]
    recurrent = local[...] + fine_dot(reads[...], state)
    first = iota((ROWS, 128), 1) < HD

    def head_mean(values):
        one = jnp.sum(jnp.where(first, values, 0.0), axis=1, keepdims=True)
        two = jnp.sum(jnp.where(first, 0.0, values), axis=1, keepdims=True)
        return jnp.where(first, one, two) * (1.0 / HD)

    centered = recurrent - head_mean(recurrent)
    normal = centered * lax.rsqrt(head_mean(centered * centered) + GROUP_EPS)
    mix_ref[:, 0:128] = normal.astype(BF16)

    for copy in o_copies:
        copy.wait_recv()
    for n in range(3):
        head_out = head_out + orecv[n].astype(F32)
    head_out = head_out * lax.rsqrt(
        jnp.mean(head_out * head_out, axis=0, keepdims=True) + HEAD_EPS
    )
    mix_ref[:, 128:256] = jnp.transpose(head_out).astype(BF16)

    part_rows = ROWS // (NY * NC)
    order = [across, up, down, y]

    def rows_for(core):
        return jnp.concatenate(
            [
                mix_ref[pl.ds(pl.multiple_of((n * 2 + core) * part_rows, part_rows), part_rows), :]
                for n in order
            ],
            0,
        )

    theirs = rows_for(other)
    ours = rows_for(c)
    for t in range(8):
        cols = slice(t * 256, (t + 1) * 256)
        psend[:, cols] = dot(theirs, out_w[:, cols]).astype(BF16)
    pairs = [
        send(psend.at[pl.ds(n * part_rows, part_rows)], precv.at[pl.ds(n * part_rows, part_rows)], to_other)
        for n in range(4)
    ]
    for t in range(8):
        cols = slice(t * 256, (t + 1) * 256)
        pair[:, cols] = dot(ours, out_w[:, cols])
    one, two = slice(0, D // 2), slice(D // 2, D)

    def summed(n, half):
        at = slice(n * part_rows, (n + 1) * part_rows)
        return pair[at, half] + precv[at, half].astype(F32)

    pairs[0].wait_recv()
    hsend[0] = summed(0, one).astype(BF16)
    relay_up = send(hsend.at[0], hrecv.at[0], to_up)
    hsend[1] = summed(0, two).astype(BF16)
    relay_down = send(hsend.at[1], hrecv.at[1], to_down)
    pairs[1].wait_recv()
    hsend[2] = summed(1, two).astype(BF16)
    plain_up = send(hsend.at[2], hrecv.at[2], to_up)
    pairs[2].wait_recv()
    hsend[3] = summed(2, one).astype(BF16)
    plain_down = send(hsend.at[3], hrecv.at[3], to_down)
    relay_up.wait_recv()
    hsend[4] = (summed(1, one) + hrecv[0].astype(F32)).astype(BF16)
    merged_up = send(hsend.at[4], hrecv.at[4], to_up)
    relay_down.wait_recv()
    hsend[5] = (summed(2, two) + hrecv[1].astype(F32)).astype(BF16)
    merged_down = send(hsend.at[5], hrecv.at[5], to_down)
    pairs[3].wait_recv()
    plain_up.wait_recv()
    plain_down.wait_recv()
    left_half = summed(3, one) + hrecv[3].astype(F32)
    right_half = summed(3, two) + hrecv[2].astype(F32)
    merged_up.wait_recv()
    merged_down.wait_recv()
    left_half = left_half + hrecv[4].astype(F32)
    right_half = right_half + hrecv[5].astype(F32)
    total = jnp.sum(left_half * left_half, axis=1, keepdims=True) + jnp.sum(
        right_half * right_half, axis=1, keepdims=True
    )
    scale = lax.rsqrt(total * (1.0 / D) + NORM_EPS)
    out_ref[:, one] = (left_half * scale * out_gain_ref[:, one]).astype(BF16)
    out_ref[:, two] = (right_half * scale * out_gain_ref[:, two]).astype(BF16)
    for copy in courier.copies:
        copy.wait_send()
    for n in range(1, NZ):

        @pl.when(z + n < NZ)
        def _(n=n):
            gz_copies[n - 1].wait_send()


def run_layer(lam, hid, gain, up, base, shift, rate, wr, wa, out_gain, weights):
    whole = pl.BlockSpec(memory_space=VMEM)
    far = pl.BlockSpec(memory_space=pl.ANY)
    share = ROWS // (NY * NC)
    count = 13 + 16 + 3 + 3 + 3 + 3 + 10 + 7
    rows = VMEM((ROWS, 128), BF16)
    return pl.pallas_call(
        layer,
        out_shape=(
            jax.ShapeDtypeStruct((share, D), BF16),
            jax.ShapeDtypeStruct((1, 2, ROWS), F32),
        ),
        in_specs=[pl.BlockSpec(memory_space=pltpu.SMEM)] + [far] * 16,
        out_specs=(whole, whole),
        scratch_shapes=[
            VMEM((NY * NC, ROWS, FEAT), BF16),
            VMEM((D, 896), BF16),
            VMEM((ROWS, 896), F32),
            VMEM((ROWS, 128), F32),
            VMEM((1, D), F32),
            VMEM((128, 128), BF16),
            VMEM((1, 128), F32),
            VMEM((ROWS, 128), F32),
            VMEM((1, 128), F32),
            VMEM((256, D), BF16),
            VMEM((1, D), F32),
            rows,
            rows,
            VMEM((128, ROWS), BF16),
            rows,
            rows,
            rows,
            VMEM((ROWS, 128), F32),
            VMEM((7, ROWS, 128), BF16),
            VMEM((7, 128, ROWS), BF16),
            VMEM((NX, ROWS, 128), BF16),
            VMEM((NX, 2 * ROWS, 128), BF16),
            VMEM((NX, 128, 2 * ROWS), F32),
            VMEM((NX, 8, 2 * ROWS), F32),
            VMEM((NX, 8, 2 * ROWS), F32),
            VMEM((3, 128, ROWS), BF16),
            VMEM((3, 128, ROWS), BF16),
            VMEM((NX, 2 * ROWS), F32),
            VMEM((3, NX, 2 * ROWS), F32),
            VMEM((NX, 2 * ROWS), F32),
            VMEM((NX, 2 * ROWS), F32),
            VMEM((HD, 256), F32),
            VMEM((NX, HD, 256), F32),
            VMEM((HD, 256), BF16),
            VMEM((NZ, HD, 256), BF16),
            VMEM((ROWS, 128), F32),
            VMEM((ROWS, 128), F32),
            VMEM((128, 128), F32),
            VMEM((ROWS, 256), BF16),
            VMEM((4 * share, D), BF16),
            VMEM((4 * share, D), BF16),
            VMEM((4 * share, D), F32),
            VMEM((6, share, D // 2), BF16),
            VMEM((6, share, D // 2), BF16),
            pltpu.SemaphoreType.DMA((16,)),
            pltpu.SemaphoreType.DMA((count,)),
            pltpu.SemaphoreType.DMA((count,)),
        ],
        compiler_params=pltpu.CompilerParams(
            collective_id=0, has_side_effects=True, vmem_limit_bytes=63 * 2**20
        ),
        name="layer",
    )(lam, hid, gain, up, base, shift, rate, wr, wa, out_gain, *weights)


def per_device(
    hidden_in,
    in_gain,
    receptance_weight,
    key_weight,
    value_weight,
    decay_down,
    decay_up,
    decay_base,
    decay_shift,
    learn_rate,
    query_pair,
    key_pair,
    value_pair,
    mix_lambda,
    out_recurrent,
    out_attention,
    out_gain,
):
    layer_out, sums = run_layer(
        mix_lambda,
        hidden_in,
        in_gain.reshape(1, D),
        decay_up,
        decay_base.reshape(1, 128),
        decay_shift,
        learn_rate.reshape(1, 128),
        out_recurrent,
        out_attention,
        out_gain.reshape(1, D),
        (
            receptance_weight,
            key_weight,
            value_weight,
            decay_down,
            query_pair.reshape(D, 128),
            key_pair.reshape(D, 128),
            value_pair.reshape(D, 128),
        ),
    )
    return layer_out, sums


def solution(mesh):
    split_mesh = Mesh(mesh.devices.reshape(NZ, NX, NY, NC), ("z", "x", "y", "c"))
    sp, tp = ("z", "x"), ("y", "c")
    placed = (
        P(sp, tp),
        P(),
        P(None, tp),
        P(None, tp),
        P(None, tp),
        P(),
        P(None, tp),
        P(tp),
        P(sp, tp),
        P(tp),
        P(None, tp, None),
        P(None, tp, None),
        P(None, tp, None),
        P(tp),
        P(tp, None),
        P(tp, None),
        P(),
    )
    return jax.shard_map(
        per_device,
        mesh=split_mesh,
        in_specs=placed,
        out_specs=(P((*sp, *tp), None), P(tp, None, sp)),
        check_vma=False,
    )
```

```python
import functools
import math

import jax
import jax.numpy as jnp
from jax import lax
from jax.experimental import pallas as pl
from jax.experimental.pallas import tpu as pltpu
from jax.sharding import Mesh
from jax.sharding import PartitionSpec as P

F32 = jnp.float32
BF16 = jnp.bfloat16
HD = 64
NZ, NX, NY, NC = 8, 4, 4, 2
ROWS = 384
HALF = ROWS // 2
D = 2048
FEAT = 256
CHUNK = 128
SUB = 32
DECAY_SCALE = math.exp(-0.5)
NORM_EPS = 1e-06
GROUP_EPS = 0.00064
HEAD_EPS = 1e-05
KEY_EPS = 1e-06
NEGATIVE = -1e30
TINY = 1e-37
LOG2E = 1.4426950408889634
LN2 = 0.6931471805599453
MESH = pl.DeviceIdType.MESH
VMEM = pltpu.VMEM
HIGHEST = lax.Precision.HIGHEST


def dot(a, b):
    return jnp.dot(a, b, preferred_element_type=F32)


def dot_nt(a, b):
    return lax.dot_general(a, b, (((1,), (1,)), ((), ())), preferred_element_type=F32)


def split(x):
    high = x.astype(BF16)
    return high, (x - high.astype(F32)).astype(BF16)


def fine_dot(a, b):
    a_high, a_low = split(a)
    b_high, b_low = split(b)
    both = dot(jnp.concatenate([a_high, a_low], 1), jnp.concatenate([b_high, b_high], 0))
    return both + dot(a_high, b_low)


def fine_dot_nt(a, b):
    a_high, a_low = split(a)
    b_high, b_low = split(b)
    both = dot_nt(jnp.concatenate([a_high, a_low], 1), jnp.concatenate([b_high, b_high], 1))
    return both + dot_nt(a_high, b_low)


def coarse_dot(a, b):
    return dot(a.astype(BF16), b.astype(BF16))


def remote(src, dst, send_sem, recv_sem, where):
    return pltpu.make_async_remote_copy(
        src_ref=src,
        dst_ref=dst,
        send_sem=send_sem,
        recv_sem=recv_sem,
        device_id=where,
        device_id_type=MESH,
    )


def greet(places):
    barrier = pltpu.get_barrier_semaphore()
    for place in places:
        pl.semaphore_signal(barrier, inc=1, device_id=place, device_id_type=MESH)
    pl.semaphore_wait(barrier, len(places))


def iota(shape, dim):
    return lax.broadcasted_iota(jnp.int32, shape, dim)


def by_head(x):
    first = lax.rem(iota(x.shape, 1), 128) < HD
    zero = jnp.zeros_like(x)
    return jnp.concatenate([jnp.where(first, x, zero), jnp.where(first, zero, x)], 0)


def same_head(shape):
    return (iota(shape, 0) < HD) == (lax.rem(iota(shape, 1), 128) < HD)


SIZES = ((1, 8), (8, 32), (32, 128))


def blocks_mask(small, large):
    row, col = iota((CHUNK, CHUNK), 0), iota((CHUNK, CHUNK), 1)
    return (lax.div(row, large) == lax.div(col, large)) & (lax.div(row, small) > lax.div(col, small))


def inverses(lowers):
    row, col = iota((CHUNK, CHUNK), 0), iota((CHUNK, CHUNK), 1)
    identity = jnp.where(row == col, 1.0, 0.0)
    found = None
    for small, large in SIZES:
        keep = blocks_mask(small, large)
        parts = [jnp.where(keep, lower, 0.0) for lower in lowers]
        if found is None:
            steps = parts
            found = [identity + part for part in parts]
        else:
            steps = [coarse_dot(f, part) for f, part in zip(found, parts)]
            found = [f + coarse_dot(s, f) for f, s in zip(found, steps)]
        reach = 2
        while reach * small < large:
            steps = [coarse_dot(s, s) for s in steps]
            found = [f + coarse_dot(s, f) for f, s in zip(found, steps)]
            reach *= 2
    return found


def all_terms(receptance, keys, values, decays, rate):
    count = ROWS // CHUNK
    cuts = [slice(n * CHUNK, (n + 1) * CHUNK) for n in range(count)]
    row, col = iota((CHUNK, CHUNK), 0), iota((CHUNK, CHUNK), 1)
    ones = (row >= col).astype(BF16)
    first = col < HD
    w = [decays[at, :] for at in cuts]
    r = [receptance[at, :].astype(F32) for at in cuts]
    k = [keys[at, :].astype(F32) for at in cuts]
    v = [values[at, :] for at in cuts]
    running = []
    for part in w:
        high = part.astype(BF16)
        rest = part - high.astype(F32)
        middle = rest.astype(BF16)
        lowest = (rest - middle.astype(F32)).astype(BF16)
        running.append(
            dot(jnp.concatenate([ones, ones], 1), jnp.concatenate([high, middle], 0))
            + dot(ones, lowest)
        )
    before = [a - b for a, b in zip(running, w)]
    ending = [a[CHUNK - 1 :, :] for a in running]
    unit = []
    for part in k:
        square = part * part
        one = jnp.sum(jnp.where(first, square, 0.0), axis=1, keepdims=True)
        two = jnp.sum(jnp.where(first, 0.0, square), axis=1, keepdims=True)
        unit.append(part * lax.rsqrt(jnp.where(first, one, two) + KEY_EPS))
    erasing = [u * rate for u in unit]
    pieces = [[] for _ in cuts]
    for i in range(CHUNK // SUB):
        at = slice(i * SUB, (i + 1) * SUB)
        for n in range(count):
            start = running[n][i * SUB - 1 : i * SUB, :] if i else jnp.zeros_like(ending[n])
            left = jnp.concatenate(
                [
                    -unit[n][at] * jnp.exp(before[n][at] - start),
                    r[n][at] * jnp.exp(running[n][at] - start),
                ],
                0,
            )
            growth = jnp.exp(jnp.where(row < (i + 1) * SUB, start - running[n], -100.0))
            right = jnp.concatenate([erasing[n] * growth, k[n] * growth], 0)
            pieces[n].append(fine_dot_nt(by_head(left), right))

    def matrix(n, head, read, which, keep):
        at = head * 2 * SUB + read * SUB
        whole = jnp.concatenate(
            [p[at : at + SUB, which * CHUNK : (which + 1) * CHUNK] for p in pieces[n]], 0
        )
        return jnp.where(keep, whole, 0.0)

    strict, causal = row > col, row >= col
    found = inverses([matrix(n, h, 0, 0, strict) for n in range(count) for h in range(2)])
    found = [jnp.concatenate(found[2 * n : 2 * n + 2], 1) for n in range(count)]

    def pair(n, read, which, keep):
        return jnp.concatenate(
            [matrix(n, h, read, which, keep).astype(BF16) for h in range(2)], 1
        )

    by_value = [by_head(part) for part in v]
    carried = [dot(pair(n, 0, 1, strict), by_value[n]) for n in range(count)]
    right_side = [
        by_head(jnp.concatenate([-unit[n] * jnp.exp(before[n]), carried[n]], 1))
        for n in range(count)
    ]
    solved = [fine_dot(found[n], right_side[n]) for n in range(count)]
    seen = [
        dot(pair(n, 1, 0, causal), by_head(solved[n].astype(BF16))) for n in range(count)
    ]
    local = [seen[n][:, 128:] + dot(pair(n, 1, 1, causal), by_value[n]) for n in range(count)]
    read_state = [r[n] * jnp.exp(running[n]) + seen[n][:, :128] for n in range(count)]
    none = jnp.zeros((CHUNK, 128), F32)
    wide_row, wide_col = iota((128, 256), 0), iota((128, 256), 1)
    steps = []
    for n in range(count):
        to_end = jnp.exp(ending[n] - running[n])
        left = jnp.concatenate(
            [jnp.transpose(erasing[n] * to_end), jnp.transpose(k[n] * to_end)], 1
        )
        right = jnp.concatenate(
            [solved[n], jnp.concatenate([none, v[n].astype(F32)], 1)], 0
        )
        step = jnp.where(same_head((128, 256)), fine_dot(left, right), 0.0)
        decayed = jnp.concatenate(
            [jnp.broadcast_to(jnp.exp(ending[n]), (128, 128)), none], 1
        )
        steps.append(step + jnp.where(wide_row == wide_col, decayed, 0.0))
    return read_state, local, steps


def device_terms(receptance, keys, values, decays, rate):
    read_state, local, steps = all_terms(receptance, keys, values, decays, rate)
    reads, reach = [read_state[0]], [local[0]]
    so_far = steps[0]
    for n in range(1, len(steps)):
        seen = fine_dot(read_state[n], so_far)
        reads.append(seen[:, :128])
        reach.append(local[n] + seen[:, 128:])
        so_far = compose(steps[n], so_far)
    return reads, reach, so_far


def compose(later, earlier):
    out = fine_dot(later[:, :128], earlier)
    none = jnp.zeros((128, 128), F32)
    return out + jnp.concatenate([none, later[:, 128:]], 1)


def packed(step):
    return step[:HD] + step[HD:]


def unpacked(step):
    both = jnp.concatenate([step, step], 0)
    return jnp.where(same_head((128, 256)), both, 0.0)


def packed_identity():
    row, col = iota((HD, 256), 0), iota((HD, 256), 1)
    return jnp.where((col < 128) & (lax.rem(col, HD) == row), 1.0, 0.0)


class Courier:
    def __init__(self, ssem, rsem):
        self.ssem, self.rsem, self.copies = ssem, rsem, []

    def make(self, src, dst, where):
        n = len(self.copies)
        copy = remote(src, dst, self.ssem.at[n], self.rsem.at[n], where)
        self.copies.append(copy)
        return copy

    def send(self, src, dst, where):
        copy = self.make(src, dst, where)
        copy.start()
        return copy


def load_all(places, sems, first):
    loads = []
    for n, (src, dst) in enumerate(places):
        load = pltpu.make_async_copy(src, dst, sems.at[first + n])
        load.start()
        loads.append(load)
    return loads


def layer(
    lam_ref,
    hid_hbm,
    gain_hbm,
    up_hbm,
    base_hbm,
    shift_hbm,
    rate_hbm,
    wr_hbm,
    wa_hbm,
    out_gain_hbm,
    *rest,
):
    weights = rest[:7]
    out_ref, sums_ref = rest[7:9]
    (
        hbuf,
        wbuf,
        proj,
        sumsq,
        gain_ref,
        up_ref,
        base_ref,
        shift_ref,
        rate_ref,
        out_w,
        out_gain_ref,
        q_ref,
        k_ref,
        vt_ref,
        r_ref,
        rk_ref,
        rv_ref,
        ld_ref,
        kbuf,
        vbuf,
        qbuf,
        qwide,
        acc,
        top,
        low,
        osend,
        orecv,
        stsend,
        strecv,
        joined,
        weigh,
        gxsend,
        gxbuf,
        gzsend,
        gzbuf,
        reads,
        local,
        state_ref,
        mix_ref,
        psend,
        precv,
        pair,
        hsend,
        hrecv,
        wsem,
        ssem,
        rsem,
    ) = rest[9:]
    z = lax.axis_index("z")
    x = lax.axis_index("x")
    y = lax.axis_index("y")
    c = lax.axis_index("c")
    other = 1 - c
    up, down, across = lax.rem(y + 1, NY), lax.rem(y + 3, NY), lax.rem(y + 2, NY)
    own = y * 2 + c
    loads = load_all([(hid_hbm, hbuf.at[own])], wsem, 0)
    places = [(w, wbuf.at[:, pl.ds(n * 128, 128)]) for n, w in enumerate(weights)]
    places += [
        (gain_hbm, gain_ref),
        (up_hbm, up_ref),
        (base_hbm, base_ref),
        (shift_hbm, shift_ref),
        (rate_hbm, rate_ref),
        (wr_hbm, out_w.at[pl.ds(0, 128)]),
        (wa_hbm, out_w.at[pl.ds(128, 128)]),
        (out_gain_hbm, out_gain_ref),
    ]
    loads += load_all(places, wsem, 1)
    to_up, to_down, to_other = {"y": up}, {"y": down}, {"c": other}
    z_up, z_down = {"z": lax.rem(z + 1, NZ)}, {"z": lax.rem(z + NZ - 1, NZ)}
    z_others = [{"z": lax.rem(z + n, NZ)} for n in range(1, NZ)]
    x_others = [lax.rem(x + n, NX) for n in range(1, NX)]
    greet([to_up, to_down, to_other, z_up, z_down] + [{"x": n} for n in x_others])
    courier = Courier(ssem, rsem)
    send = courier.send
    loads[0].wait()

    first, second = pl.ds(0, HALF), pl.ds(HALF, HALF)

    def share(number, part, where):
        block = hbuf.at[number]
        if part is not None:
            block = block.at[part]
        return send(block, block, where)

    below, above, far = down * 2 + c, up * 2 + c, across * 2 + c
    below_first = share(own, first, to_up)
    above_second = share(own, second, to_down)
    below_second = share(own, second, to_up)
    above_first = share(own, first, to_down)
    beside = share(own, None, to_other)
    for load in loads[1:]:
        load.wait()

    def add(number, fresh=False, cols=slice(0, 896), squared=True):
        block = hbuf.at[number]
        at = pl.multiple_of(number * FEAT, FEAT)
        w = wbuf[pl.ds(at, FEAT), cols]
        gain = gain_ref[:, pl.ds(at, FEAT)]

        for t in range(ROWS // 128):
            rows = pl.ds(t * 128, 128)
            h = block[rows, :].astype(F32)
            squares = h[:, :128] * h[:, :128] + h[:, 128:] * h[:, 128:]
            product = dot((h * gain).astype(BF16), w)
            if fresh:
                sumsq[rows, :] = squares
                proj[rows, :] = product
            else:
                if squared:
                    sumsq[rows, :] += squares
                proj[rows, cols] += product

    add(own, True)
    beside.wait_recv()
    add(y * 2 + other)
    below_first.wait_recv()
    far_first = share(below, first, to_up)
    relays = [share(below, first, to_other)]
    above_second.wait_recv()
    far_second = share(above, second, to_down)
    relays.append(share(above, second, to_other))
    below_second.wait_recv()
    relays.append(share(below, second, to_other))
    above_first.wait_recv()
    relays.append(share(above, first, to_other))
    add(below)
    add(above)
    far_first.wait_recv()
    relays.append(share(far, first, to_other))
    far_second.wait_recv()
    relays.append(share(far, second, to_other))
    relays[0].wait_recv()
    relays[2].wait_recv()
    add(down * 2 + other)
    relays[1].wait_recv()
    relays[3].wait_recv()
    add(up * 2 + other)
    add(far)
    relays[4].wait_recv()
    relays[5].wait_recv()
    add(across * 2 + other, cols=slice(512, 896))

    total = jnp.sum(sumsq[...], axis=1, keepdims=True)
    scale = lax.rsqrt(total * (1.0 / D) + NORM_EPS)
    k_ref[...] = (proj[:, 640:768] * scale).astype(BF16)
    vt_ref[...] = jnp.transpose(proj[:, 768:896] * scale).astype(BF16)
    q_ref[...] = (proj[:, 512:640] * (scale * (LOG2E * HD**-0.5))).astype(BF16)

    def pass_on(buf, source, slot, first, second):
        ahead = courier.make(
            buf.at[slot - 1, first], buf.at[slot if slot < 3 else 6, first], z_up
        )
        back = courier.make(buf.at[slot + 2, second], buf.at[slot + 3, second], z_down)

        def forth(n, copy):
            source[n].wait_recv()
            copy.start()

        @pl.when(z < 3)
        def _():
            forth(1, back)
            forth(0, ahead)

        @pl.when(z >= 3)
        def _():
            forth(0, ahead)
            forth(1, back)

        return ahead, back

    key_all, value_all = pl.ds(0, ROWS), pl.ds(0, 128)
    keys = (send(k_ref, kbuf.at[0], z_up), send(k_ref, kbuf.at[3], z_down))
    values = (send(vt_ref, vbuf.at[0], z_up), send(vt_ref, vbuf.at[3], z_down))
    q_copies = [send(q_ref, qbuf.at[x], {"x": x_others[n]}) for n in (1, 0, 2)]

    add(across * 2 + other, cols=slice(0, 512), squared=False)

    @pl.loop(0, ROWS // 128)
    def _(t):
        rows = pl.ds(pl.multiple_of(t * 128, 128), 128)
        total = jnp.sum(sumsq[rows, :], axis=1, keepdims=True)
        scale = lax.rsqrt(total * (1.0 / D) + NORM_EPS)
        r_ref[rows, :] = (proj[rows, 0:128] * scale).astype(BF16)
        rk_ref[rows, :] = (proj[rows, 128:256] * scale).astype(BF16)
        rv_ref[rows, :] = (proj[rows, 256:384] * scale).astype(BF16)
        down_low = jnp.tanh(proj[rows, 384:512] * scale).astype(BF16)
        gate = dot(down_low, up_ref[...]) + base_ref[...]
        ld_ref[rows, :] = -DECAY_SCALE * jax.nn.sigmoid(gate) + shift_ref[rows, :]

    found_reads, found_local, so_far = device_terms(r_ref, rk_ref, rv_ref, ld_ref, rate_ref[...])
    for n in range(ROWS // CHUNK):
        reads[n * CHUNK : (n + 1) * CHUNK, :] = found_reads[n]
        local[n * CHUNK : (n + 1) * CHUNK, :] = found_local[n]
    gxsend[...] = packed(so_far)
    gxbuf[x] = packed(so_far)
    gx_copies = [send(gxsend, gxbuf.at[x], {"x": n}) for n in x_others]

    keys = pass_on(kbuf, keys, 1, key_all, key_all)
    values = pass_on(vbuf, values, 1, value_all, value_all)

    qbuf[x] = q_ref[...]
    for copy in q_copies:
        copy.wait_recv()
    for j in range(NX):
        qwide[j] = by_head(qbuf[j])
    tiles = [slice(t * 256, (t + 1) * 256) for t in range(3)]

    def attend_all(blocks, own):
        k_all = [k_block[...] for k_block, _ in blocks]
        v_all = jnp.concatenate([v_block[...] for _, v_block in blocks], 1)

        def scores_of(j):
            found = [[dot_nt(k, qwide[j, cols, :]) for k in k_all] for cols in tiles]
            if own:
                for t in range(3):
                    key_at = iota((ROWS, 256), 0)
                    query_at = lax.rem(iota((ROWS, 256), 1) + t * 256, ROWS)
                    keep = query_at - key_at >= (x - j) * ROWS
                    found[t] = [jnp.where(keep, s, NEGATIVE) for s in found[t]]
            return found, [
                functools.reduce(
                    jnp.maximum, [jnp.max(s, axis=0, keepdims=True) for s in group]
                )
                for group in found
            ]

        ready = scores_of(0)
        for j in range(NX):
            following = scores_of(j + 1) if j + 1 < NX else None
            scores, highest = ready
            if not own:
                olds = [top[j, 0:1, cols] for cols in tiles]
                sums = [low[j, 0:1, cols] for cols in tiles]
                totals = [acc[j, :, cols] for cols in tiles]
            for t, cols in enumerate(tiles):
                new = highest[t] if own else jnp.maximum(olds[t], highest[t])
                weights = [jnp.exp2(s - new) for s in scores[t]]
                part = sum(jnp.sum(w, axis=0, keepdims=True) for w in weights)
                seen = dot(v_all, jnp.concatenate([w.astype(BF16) for w in weights], 0))
                top[j, 0:1, cols] = new
                if own:
                    low[j, 0:1, cols] = part
                    acc[j, :, cols] = seen
                else:
                    rescale = jnp.exp2(olds[t] - new)
                    low[j, 0:1, cols] = sums[t] * rescale + part
                    acc[j, :, cols] = totals[t] * rescale + seen
            ready = following

    def attend(slots, needed):
        @pl.when(needed)
        def _():
            attend_all([(kbuf.at[slot], vbuf.at[slot]) for slot in slots], False)

    attend_all([(k_ref, vt_ref)], True)
    keys = pass_on(kbuf, keys, 2, key_all, key_all)
    attend([0, 3], z == NZ - 1)
    attend([0], (z >= 1) & (z < NZ - 1))
    values = pass_on(vbuf, values, 2, value_all, value_all)

    for copy in gx_copies:
        copy.wait_recv()
    none = jnp.zeros((128, 128), F32)
    identity = jnp.where(iota((128, 256), 0) == iota((128, 256), 1), 1.0, 0.0)
    before_x = identity
    total = unpacked(gxbuf[0])
    for n in range(1, NX):
        before_x = jnp.where(x == n, total, before_x)
        total = compose(unpacked(gxbuf[n]), total)
    share = (packed(total) - packed_identity()).astype(BF16)
    gzsend[...] = share
    gzbuf[z] = share

    keys = pass_on(kbuf, keys, 3, pl.ds(0, HALF), pl.ds(HALF, HALF))
    attend([1, 4], z >= NZ - 2)
    attend([1], (z >= 2) & (z < NZ - 2))
    values = pass_on(vbuf, values, 3, pl.ds(0, HD), pl.ds(HD, HD))
    attend([2, 5], z >= NZ - 3)
    attend([2], (z >= 3) & (z < NZ - 3))
    gz_copies = []
    for n in range(1, NZ):
        at = 50 + n
        gz_copies.append(
            remote(gzsend, gzbuf.at[z], ssem.at[at], rsem.at[at], {"z": lax.rem(z + n, NZ)})
        )

    def finish_ring():
        for copy in (*keys, *values):
            copy.wait_recv()
        for n in range(1, NZ):

            @pl.when(z + n < NZ)
            def _(n=n):
                gz_copies[n - 1].start()

    @pl.when(z >= 4)
    def _():
        finish_ring()
        attend_all([(kbuf.at[6], vbuf.at[6])], False)

    totals = jnp.maximum(jnp.concatenate([low[j, 0:1, :] for j in range(NX)], 0), TINY)
    level = jnp.concatenate([top[j, 0:1, :] for j in range(NX)], 0) + jnp.log2(totals)
    stsend[...] = level
    st_copies = [send(stsend, strecv.at[n], {"x": x_others[n]}) for n in (1, 0, 2)]

    @pl.when(z < 4)
    def _():
        finish_ring()

    for copy in st_copies:
        copy.wait_recv()
    theirs = [strecv[n] for n in range(3)]
    highest = functools.reduce(jnp.maximum, theirs, level)
    whole = sum((jnp.exp2(one - highest) for one in theirs), jnp.exp2(level - highest))
    joint = highest + jnp.log2(whole)
    joined[...] = joint
    weigh[...] = jnp.exp2(level - joint) / totals

    def contribution(j):
        w = weigh[pl.ds(j, 1), :]
        part = acc[j]
        return part[:, :ROWS] * w[:, :ROWS] - part[:, ROWS:] * (lam_ref[0] * w[:, ROWS:])

    o_copies = []
    for n in (1, 0, 2):
        osend[n] = contribution(x_others[n]).astype(BF16)
        o_copies.append(send(osend.at[n], orecv.at[n], {"x": x_others[n]}))
    head_out = contribution(x)
    sums = joined[pl.ds(x, 1), :] * LN2
    sums_ref[0, 0:1, :] = sums[:, :ROWS]
    sums_ref[0, 1:2, :] = sums[:, ROWS:]

    for n in range(1, NZ):

        @pl.when(z >= n)
        def _(n=n):
            gz_copies[n - 1].wait_recv()

    state_ref[...] = none
    for n in range(NZ - 1):

        @pl.when(n < z)
        def _(n=n):
            step = unpacked(gzbuf[n].astype(F32) + packed_identity())
            state_ref[...] = fine_dot(step[:, :128], state_ref[...]) + step[:, 128:]

    state = fine_dot(before_x[:, :128], state_ref[...]) + before_x[:, 128:]
    recurrent = local[...] + fine_dot(reads[...], state)
    first = iota((ROWS, 128), 1) < HD

    def head_mean(values):
        one = jnp.sum(jnp.where(first, values, 0.0), axis=1, keepdims=True)
        two = jnp.sum(jnp.where(first, 0.0, values), axis=1, keepdims=True)
        return jnp.where(first, one, two) * (1.0 / HD)

    centered = recurrent - head_mean(recurrent)
    normal = centered * lax.rsqrt(head_mean(centered * centered) + GROUP_EPS)
    mix_ref[:, 0:128] = normal.astype(BF16)

    for copy in o_copies:
        copy.wait_recv()
    for n in range(3):
        head_out = head_out + orecv[n].astype(F32)
    head_out = head_out * lax.rsqrt(
        jnp.mean(head_out * head_out, axis=0, keepdims=True) + HEAD_EPS
    )
    mix_ref[:, 128:256] = jnp.transpose(head_out).astype(BF16)

    part_rows = ROWS // (NY * NC)
    order = [across, up, down, y]

    def rows_for(core):
        return jnp.concatenate(
            [
                mix_ref[pl.ds(pl.multiple_of((n * 2 + core) * part_rows, part_rows), part_rows), :]
                for n in order
            ],
            0,
        )

    theirs = rows_for(other)
    ours = rows_for(c)
    for t in range(8):
        cols = slice(t * 256, (t + 1) * 256)
        psend[:, cols] = dot(theirs, out_w[:, cols]).astype(BF16)
    pairs = [
        send(psend.at[pl.ds(n * part_rows, part_rows)], precv.at[pl.ds(n * part_rows, part_rows)], to_other)
        for n in range(4)
    ]
    for t in range(8):
        cols = slice(t * 256, (t + 1) * 256)
        pair[:, cols] = dot(ours, out_w[:, cols])
    one, two = slice(0, D // 2), slice(D // 2, D)

    def summed(n, half):
        at = slice(n * part_rows, (n + 1) * part_rows)
        return pair[at, half] + precv[at, half].astype(F32)

    pairs[0].wait_recv()
    hsend[0] = summed(0, one).astype(BF16)
    relay_up = send(hsend.at[0], hrecv.at[0], to_up)
    hsend[1] = summed(0, two).astype(BF16)
    relay_down = send(hsend.at[1], hrecv.at[1], to_down)
    pairs[1].wait_recv()
    hsend[2] = summed(1, two).astype(BF16)
    plain_up = send(hsend.at[2], hrecv.at[2], to_up)
    pairs[2].wait_recv()
    hsend[3] = summed(2, one).astype(BF16)
    plain_down = send(hsend.at[3], hrecv.at[3], to_down)
    relay_up.wait_recv()
    hsend[4] = (summed(1, one) + hrecv[0].astype(F32)).astype(BF16)
    merged_up = send(hsend.at[4], hrecv.at[4], to_up)
    relay_down.wait_recv()
    hsend[5] = (summed(2, two) + hrecv[1].astype(F32)).astype(BF16)
    merged_down = send(hsend.at[5], hrecv.at[5], to_down)
    pairs[3].wait_recv()
    plain_up.wait_recv()
    plain_down.wait_recv()
    left_half = summed(3, one) + hrecv[3].astype(F32)
    right_half = summed(3, two) + hrecv[2].astype(F32)
    merged_up.wait_recv()
    merged_down.wait_recv()
    left_half = left_half + hrecv[4].astype(F32)
    right_half = right_half + hrecv[5].astype(F32)
    total = jnp.sum(left_half * left_half, axis=1, keepdims=True) + jnp.sum(
        right_half * right_half, axis=1, keepdims=True
    )
    scale = lax.rsqrt(total * (1.0 / D) + NORM_EPS)
    out_ref[:, one] = (left_half * scale * out_gain_ref[:, one]).astype(BF16)
    out_ref[:, two] = (right_half * scale * out_gain_ref[:, two]).astype(BF16)
    for copy in courier.copies:
        copy.wait_send()
    for n in range(1, NZ):

        @pl.when(z + n < NZ)
        def _(n=n):
            gz_copies[n - 1].wait_send()


def run_layer(lam, hid, gain, up, base, shift, rate, wr, wa, out_gain, weights):
    whole = pl.BlockSpec(memory_space=VMEM)
    far = pl.BlockSpec(memory_space=pl.ANY)
    share = ROWS // (NY * NC)
    count = 13 + 16 + 3 + 3 + 3 + 3 + 10 + 7
    rows = VMEM((ROWS, 128), BF16)
    return pl.pallas_call(
        layer,
        out_shape=(
            jax.ShapeDtypeStruct((share, D), BF16),
            jax.ShapeDtypeStruct((1, 2, ROWS), F32),
        ),
        in_specs=[pl.BlockSpec(memory_space=pltpu.SMEM)] + [far] * 16,
        out_specs=(whole, whole),
        scratch_shapes=[
            VMEM((NY * NC, ROWS, FEAT), BF16),
            VMEM((D, 896), BF16),
            VMEM((ROWS, 896), F32),
            VMEM((ROWS, 128), F32),
            VMEM((1, D), F32),
            VMEM((128, 128), BF16),
            VMEM((1, 128), F32),
            VMEM((ROWS, 128), F32),
            VMEM((1, 128), F32),
            VMEM((256, D), BF16),
            VMEM((1, D), F32),
            rows,
            rows,
            VMEM((128, ROWS), BF16),
            rows,
            rows,
            rows,
            VMEM((ROWS, 128), F32),
            VMEM((7, ROWS, 128), BF16),
            VMEM((7, 128, ROWS), BF16),
            VMEM((NX, ROWS, 128), BF16),
            VMEM((NX, 2 * ROWS, 128), BF16),
            VMEM((NX, 128, 2 * ROWS), F32),
            VMEM((NX, 8, 2 * ROWS), F32),
            VMEM((NX, 8, 2 * ROWS), F32),
            VMEM((3, 128, ROWS), BF16),
            VMEM((3, 128, ROWS), BF16),
            VMEM((NX, 2 * ROWS), F32),
            VMEM((3, NX, 2 * ROWS), F32),
            VMEM((NX, 2 * ROWS), F32),
            VMEM((NX, 2 * ROWS), F32),
            VMEM((HD, 256), F32),
            VMEM((NX, HD, 256), F32),
            VMEM((HD, 256), BF16),
            VMEM((NZ, HD, 256), BF16),
            VMEM((ROWS, 128), F32),
            VMEM((ROWS, 128), F32),
            VMEM((128, 128), F32),
            VMEM((ROWS, 256), BF16),
            VMEM((4 * share, D), BF16),
            VMEM((4 * share, D), BF16),
            VMEM((4 * share, D), F32),
            VMEM((6, share, D // 2), BF16),
            VMEM((6, share, D // 2), BF16),
            pltpu.SemaphoreType.DMA((16,)),
            pltpu.SemaphoreType.DMA((count,)),
            pltpu.SemaphoreType.DMA((count,)),
        ],
        compiler_params=pltpu.CompilerParams(
            collective_id=0, has_side_effects=True, vmem_limit_bytes=63 * 2**20
        ),
        name="layer",
    )(lam, hid, gain, up, base, shift, rate, wr, wa, out_gain, *weights)


def per_device(
    hidden_in,
    in_gain,
    receptance_weight,
    key_weight,
    value_weight,
    decay_down,
    decay_up,
    decay_base,
    decay_shift,
    learn_rate,
    query_pair,
    key_pair,
    value_pair,
    mix_lambda,
    out_recurrent,
    out_attention,
    out_gain,
):
    layer_out, sums = run_layer(
        mix_lambda,
        hidden_in,
        in_gain.reshape(1, D),
        decay_up,
        decay_base.reshape(1, 128),
        decay_shift,
        learn_rate.reshape(1, 128),
        out_recurrent,
        out_attention,
        out_gain.reshape(1, D),
        (
            receptance_weight,
            key_weight,
            value_weight,
            decay_down,
            query_pair.reshape(D, 128),
            key_pair.reshape(D, 128),
            value_pair.reshape(D, 128),
        ),
    )
    return layer_out, sums


def solution(mesh):
    split_mesh = Mesh(mesh.devices.reshape(NZ, NX, NY, NC), ("z", "x", "y", "c"))
    sp, tp = ("z", "x"), ("y", "c")
    placed = (
        P(sp, tp),
        P(),
        P(None, tp),
        P(None, tp),
        P(None, tp),
        P(),
        P(None, tp),
        P(tp),
        P(sp, tp),
        P(tp),
        P(None, tp, None),
        P(None, tp, None),
        P(None, tp, None),
        P(tp),
        P(tp, None),
        P(tp, None),
        P(),
    )
    return jax.shard_map(
        per_device,
        mesh=split_mesh,
        in_specs=placed,
        out_specs=(P((*sp, *tp), None), P(tp, None, sp)),
        check_vma=False,
    )
```
